256 devices in a mesh: fs: 16 (over y, x), tp: 16 (over z, core).
Axes of the slice: x: 4, y: 4, z: 8, core: 2. Of those that a mesh axis runs over, the one named last changes fastest.
Arguments:
- tokens: bfloat16 [2048, 4096], P('fs', 'tp'), may hold values from -6 to 6
- expert_ids: int32 [2048, 8], P('fs'), may hold values from 0 to 63, all different within a row; in each aligned block of 128 rows (0 to 127, 128 to 255, ...) at most 32 rows name the same one
- affinity: float32 [2048, 8], P('fs'), may hold values from 0.05 to 1
- norm_gain: float32 [4096], P('fs'), may hold values from 0.1 to 1.9
- gate_train: float32 [64, 512, 4096], P(None, 'tp', 'fs'), may hold values from -0.09375 to 0.09375
- up_train: float32 [64, 512, 4096], P(None, 'tp', 'fs'), may hold values from -0.09375 to 0.09375
- down_train: float32 [64, 512, 4096], P(None, 'fs', 'tp'), may hold values from -0.25 to 0.25
- shared_gate_train: float32 [512, 4096], P('tp', 'fs'), may hold values from -0.09375 to 0.09375
- shared_up_train: float32 [512, 4096], P('tp', 'fs'), may hold values from -0.09375 to 0.09375
- shared_down_train: float32 [512, 4096], P('fs', 'tp'), may hold values from -0.25 to 0.25
Outputs:
- mixed: bfloat16 [2048, 4096], P('fs', 'tp')
- gate_serve: bfloat16 [64, 512, 4096], P('fs', 'tp')
- up_serve: bfloat16 [64, 512, 4096], P('fs', 'tp')
- down_serve: bfloat16 [64, 512, 4096], P('fs', None, 'tp')
- shared_gate_serve: bfloat16 [512, 4096], P('tp')
- shared_up_serve: bfloat16 [512, 4096], P('tp')
- shared_down_serve: bfloat16 [512, 4096], P(None, 'tp')
The draws below stay inside these ranges and needn't reach their ends.
Inputs may be any that keep to these rules, and one draw needn't show every extreme that they name: `expert_ids`: each row names 8 different experts. In each aligned block of 128 rows (the tokens of one index of fs) no expert is named by more than 32 rows, a bound that some block reaches.
All inputs are finite; a program needn't handle non-finite values.
Results may differ from the reference program's by a relative error of at most 0.019.
Values may be sent and summed in bfloat16 or wider, within the bound.
A program may use at most 128 MiB of HBM per device.

```python
import math
import jax
import jax.numpy as jnp
import numpy as np
from jax import lax

D = 4096
H = 512
EXPERTS = 64
K = 8
TOK = 128
CAP = 32
TOKENS = 2048
N_FS = 16


def block_scale(own_key, dims, cuts, smallest, high):
    level = 1.0
    for dim, shards_of in cuts:
        heights = jax.random.uniform(jax.random.fold_in(jax.random.fold_in(own_key, 6), dim), (shards_of,), jnp.float32, smallest / len(cuts), high / len(cuts))
        level = level * jnp.repeat(jnp.exp(heights), dims[dim] // shards_of).reshape((-1,) + (1,) * (len(dims) - 1 - dim))
    return level


def assign_block(stream_key, own, number, rows, amount, top, reach, lean):
    order = jax.random.permutation(stream_key, amount)
    packed, usual = shares(amount, rows * top, reach, lean, True), shares(amount, rows * top, reach, lean, False)
    places = jnp.arange(amount)

    def named(tallies, rotation):
        used = int((tallies > 0).sum())
        fixed = max(1, used // 4)
        moved = fixed + (places - fixed + rotation * (used - fixed)) % max(1, amount - fixed)
        return jnp.zeros((amount,), jnp.int32).at[order[jnp.where(places < fixed, places, moved)]].set(jnp.asarray(tallies, jnp.int32))

    tallies = jnp.where(number % 4 == 0, named(packed, number // 4), named(usual, number - number // 4 - 1))
    mixed = jax.random.permutation(jax.random.fold_in(own, 3), amount)
    giver, taker = mixed[0:amount // 2 * 2:2], mixed[1:amount // 2 * 2:2]
    slack = jnp.minimum(tallies[giver] - 1, reach - tallies[taker]) // 2
    slack = jnp.where((giver == order[0]) | (taker == order[0]) | (tallies[taker] == 0), 0, jnp.maximum(slack, 0))
    moved = jax.random.randint(jax.random.fold_in(own, 4), (amount // 2,), 0, 1 << 20) % (slack + 1)
    tallies = tallies.at[giver].add(-moved).at[taker].add(moved)
    items = jnp.searchsorted(jnp.cumsum(tallies), jnp.arange(rows * top), side="right").astype(jnp.int32)
    table = items.reshape(top, rows).T
    table = table[jax.random.permutation(jax.random.fold_in(own, 1), rows)]
    rotation = jax.random.randint(jax.random.fold_in(own, 2), (rows, 1), 0, top)
    return jnp.take_along_axis(table, (jnp.arange(top)[None, :] + rotation) % top, axis=1)


def shares(count, total, limit, lean, full):
    portions = [(1 << 20) // math.isqrt(rank ** lean) + 1 for rank in range(1, count + 1)]
    largest = limit if full else min(limit, max(-(-total // count), total * portions[0] // sum(portions)))
    least = 1 if total - largest >= count - 1 else 0
    holding, spare = [largest] + [least] * (count - 1), total - largest - least * (count - 1)
    while spare > 0:
        free = [i for i in range(1, count) if holding[i] < largest] or [i for i in range(1, count) if holding[i] < limit]
        whole, left = sum([portions[i] for i in free]), spare
        for i in free:
            more = min(limit - holding[i], max(1, left * portions[i] // whole), spare)
            holding[i] = holding[i] + more
            spare = spare - more
    return np.array(holding)


def bell_draw(key, extent, scale, limit, pieces=(), kind=jnp.bfloat16):
    result = scale * jax.random.normal(key, extent, jnp.float32)
    if pieces:
        result = result * block_scale(key, extent, pieces, -0.22, 0.18)
    return jnp.clip(result, -limit, limit).astype(kind)


def setup_inputs(seed: int = 0) -> dict:
    seeds = jax.random.split(jax.random.key(seed), 11)
    tokens = bell_draw(seeds[0], (TOKENS, D), 1.0, 6.0, ((0, 16), (1, 16)))
    expert_ids_keys = jax.random.split(jax.random.fold_in(seeds[1], 1), TOKENS // TOK)
    expert_ids_turns = jax.random.permutation(jax.random.fold_in(seeds[1], 3), TOKENS // TOK)
    expert_ids = jax.vmap(lambda own, number: assign_block(jax.random.fold_in(seeds[1], 2), own, number, TOK, EXPERTS, K, CAP, 1))(expert_ids_keys, expert_ids_turns).reshape((TOKENS, K))
    affinity = jnp.clip(0.05 + 0.95 * jax.random.uniform(seeds[2], (TOKENS, K), jnp.float32) ** block_scale(seeds[2], (TOKENS, K), ((0, 16),), -0.2, 0.2), 0.05, 1.0)
    norm_gain = jnp.clip(1.0 + 0.18 * jax.random.normal(seeds[3], (D,), jnp.float32), 0.1, 1.9)
    gate_train = bell_draw(seeds[4], (EXPERTS, H, D), D ** -0.5, 0.09375, ((1, 16), (2, 16)), jnp.float32)
    up_train = bell_draw(seeds[5], (EXPERTS, H, D), D ** -0.5, 0.09375, ((1, 16), (2, 16)), jnp.float32)
    down_train = bell_draw(seeds[6], (EXPERTS, H, D), H ** -0.5, 0.25, ((1, 16), (2, 16)), jnp.float32)
    shared_gate_train = bell_draw(seeds[7], (H, D), D ** -0.5, 0.09375, ((0, 16), (1, 16)), jnp.float32)
    shared_up_train = bell_draw(seeds[8], (H, D), D ** -0.5, 0.09375, ((0, 16), (1, 16)), jnp.float32)
    shared_down_train = bell_draw(seeds[9], (H, D), H ** -0.5, 0.25, ((0, 16), (1, 16)), jnp.float32)
    return {"tokens": tokens, "expert_ids": expert_ids, "affinity": affinity, "norm_gain": norm_gain, "gate_train": gate_train, "up_train": up_train, "down_train": down_train, "shared_gate_train": shared_gate_train, "shared_up_train": shared_up_train, "shared_down_train": shared_down_train}


norm_eps = 1e-06
routed_scale = 2.5

def reference(tokens, expert_ids, affinity, norm_gain, gate_train, up_train, down_train, shared_gate_train, shared_up_train, shared_down_train):
    gain_cols = norm_gain[None, None, :]
    gate_serve = (gate_train * gain_cols).astype(jnp.bfloat16)
    up_serve = (up_train * gain_cols).astype(jnp.bfloat16)
    down_serve = down_train.astype(jnp.bfloat16)
    shared_gate_serve = (shared_gate_train * norm_gain[None, :]).astype(jnp.bfloat16)
    shared_up_serve = (shared_up_train * norm_gain[None, :]).astype(jnp.bfloat16)
    shared_down_serve = shared_down_train.astype(jnp.bfloat16)
    widened = tokens.astype(jnp.float32)
    inverse_rms = lax.rsqrt(lax.optimization_barrier(jnp.mean(widened * widened, axis=1)) + norm_eps)
    shared_gate = jnp.dot(tokens, shared_gate_serve.T, preferred_element_type=jnp.float32) * inverse_rms[:, None]
    shared_up = jnp.dot(tokens, shared_up_serve.T, preferred_element_type=jnp.float32) * inverse_rms[:, None]
    shared_hidden = (jax.nn.silu(shared_gate) * shared_up).astype(jnp.bfloat16)
    shared_out = jnp.dot(shared_hidden, shared_down_serve, preferred_element_type=jnp.float32)
    ids = expert_ids.reshape(N_FS, TOK * K)
    onehot = (ids[:, :, None] == jnp.arange(EXPERTS, dtype=jnp.int32)[None, None, :]).astype(jnp.int32)
    slot_index = lax.optimization_barrier(jnp.sum((jnp.cumsum(onehot, axis=1) - onehot) * onehot, axis=2))
    block_index = jnp.arange(N_FS, dtype=jnp.int32)[:, None]
    position = (ids * (N_FS * CAP) + block_index * CAP + slot_index).reshape(-1).astype(jnp.int32)
    token_of = jnp.repeat(jnp.arange(TOKENS, dtype=jnp.int32), K)
    rows = jnp.zeros((EXPERTS * N_FS * CAP, D), jnp.bfloat16).at[position].set(tokens[token_of])
    scales = jnp.zeros((EXPERTS * N_FS * CAP,), jnp.float32).at[position].set(inverse_rms[token_of])

    def one_expert(operands):
        rows_e, scale_e, gate_w, up_w, down_w = operands
        gate_pre = jnp.dot(rows_e, gate_w.T, preferred_element_type=jnp.float32) * scale_e[:, None]
        up_pre = jnp.dot(rows_e, up_w.T, preferred_element_type=jnp.float32) * scale_e[:, None]
        hidden = (jax.nn.silu(gate_pre) * up_pre).astype(jnp.bfloat16)
        return jnp.dot(hidden, down_w, preferred_element_type=jnp.float32).astype(jnp.bfloat16)
    outputs = lax.map(one_expert, (rows.reshape(EXPERTS, N_FS * CAP, D), scales.reshape(EXPERTS, N_FS * CAP), gate_serve, up_serve, down_serve))
    picked = outputs.reshape(EXPERTS * N_FS * CAP, D)[position].reshape(TOKENS, K, D).astype(jnp.float32)
    route_weight = routed_scale * affinity / lax.optimization_barrier(jnp.sum(affinity, axis=1, keepdims=True))
    routed = lax.optimization_barrier(jnp.sum(picked * route_weight[:, :, None], axis=1))
    mixed = (shared_out + routed).astype(jnp.bfloat16)
    return (mixed, gate_serve, up_serve, down_serve, shared_gate_serve, shared_up_serve, shared_down_serve)
```

```python
import functools

import jax
import jax.numpy as jnp
from jax import lax
from jax.experimental import pallas as pl
from jax.experimental.pallas import tpu as pltpu
from jax.sharding import PartitionSpec as P

K = 8
NORM_EPS = 1e-06
ROUTED_SCALE = 2.5
LANES = 128
F32 = jnp.float32
BF16 = jnp.bfloat16
NT_DIMS = (((1,), (1,)), ((), ()))
TN_DIMS = (((0,), (0,)), ((), ()))


def silu(v):
    return v / (1.0 + jnp.exp(-v))


def kernel(
    NF,
    NT,
    D,
    tok_ref,
    ids_ref,
    aff_ref,
    gain_ref,
    gt_ref,
    ut_ref,
    dt_ref,
    sgt_ref,
    sut_ref,
    sdt_ref,
    mixed_ref,
    gs_ref,
    us_ref,
    ds_ref,
    sgs_ref,
    sus_ref,
    sds_ref,
    wf,
    wg,
    wu,
    wd,
    ws,
    fold,
    spread_ids,
    wexp,
    idt,
    xz,
    xa,
    hv,
    hz,
    ha,
    dk,
    gsc,
    usc,
    tsc,
    asc,
    psend,
    precv,
    osend,
    orecv,
    load_sem,
    own_sem,
    ids_s,
    ids_r,
    xzs,
    xzr,
    xps,
    xpr,
    xms,
    xmr,
    hzs,
    hzr,
    hps,
    hpr,
    hms,
    hmr,
    p_s,
    p_r,
    o_s,
    o_r,
    w_s,
    w_r,
):
    f = lax.axis_index("fs")
    t = lax.axis_index("tp")
    z, c = t // 2, t % 2
    NZ = NT // 2
    TOK, DS = tok_ref.shape
    HS = sgt_ref.shape[0]
    EH = wg.shape[0]
    EP = EH // HS // NF
    GROUPS = EH // LANES
    ROWS = EP * HS

    loads = []
    for i, r in enumerate((gt_ref, ut_ref, dt_ref)):
        load = pltpu.make_async_copy(r, wf.at[i], load_sem.at[i])
        load.start()
        loads.append(load)

    bar = pltpu.get_barrier_semaphore()

    def greet_plane(i, carry):
        at = (f * 2 + c + i) % (2 * NF)
        pl.semaphore_signal(
            bar, 1, device_id={"fs": at // 2, "tp": z * 2 + at % 2},
            device_id_type=pl.DeviceIdType.MESH,
        )
        return carry

    def greet_column(i, carry):
        pl.semaphore_signal(
            bar, 1, device_id={"tp": ((z + i) % NZ) * 2 + c},
            device_id_type=pl.DeviceIdType.MESH,
        )
        return carry

    lax.fori_loop(1, 2 * NF, greet_plane, 0)
    lax.fori_loop(1, NZ, greet_column, 0)

    eye = (
        lax.broadcasted_iota(jnp.int32, (TOK, TOK), 0)
        == lax.broadcasted_iota(jnp.int32, (TOK, TOK), 1)
    ).astype(BF16)
    ids16 = jnp.concatenate([ids_ref[...].astype(F32).astype(BF16), jnp.zeros((TOK, 8), BF16)], axis=1)
    idt[f] = lax.dot_general(ids16, eye, TN_DIMS, preferred_element_type=F32).astype(BF16)

    pl.semaphore_wait(bar, 2 * NF - 1 + NZ - 1)

    def remote(src, dst, s, r, **where):
        return pltpu.make_async_remote_copy(
            src_ref=src, dst_ref=dst, send_sem=s, recv_sem=r,
            device_id=where, device_id_type=pl.DeviceIdType.MESH,
        )

    steps = [i for d in range(1, NZ // 2 + 1) for i in dict.fromkeys((d, NZ - d))]

    def along_z(src, stage, s, r):
        for i in steps:
            remote(src, stage.at[z], s.at[i], r.at[z], tp=((z + i) % NZ) * 2 + c).start()

    def in_plane(src, stage, got, zs, zr, s, r):
        for i in [0] + [(NZ - i) for i in steps]:
            zz = (z + i) % NZ
            if i:
                remote(src, stage.at[zz], zs.at[i], zr.at[zz], tp=zz * 2 + c).wait_recv()
            part = stage.at[zz] if i else src
            to = zz * 2 + c

            @pl.when(to == f)
            def _():
                got[f] = part[...]

            @pl.when(to != f)
            def _():
                remote(part, got.at[f], s.at[i], r.at[f], fs=to, tp=z * 2 + f % 2).start()

    def wait_spread_sends(src, stage, got, zs, zr, s, r):
        for i in range(NZ):
            zz = (z + i) % NZ
            to = zz * 2 + c
            if i:
                remote(src, stage.at[z], zs.at[i], zr.at[z], tp=zz * 2 + c).wait_send()

            @pl.when(to != f)
            def _():
                remote(src, got.at[f], s.at[i], r.at[f], fs=to, tp=z * 2 + f % 2).wait_send()

    def direct_block(i):
        return 2 * ((f // 2 + i) % (NF // 2)) + c

    def mate_block(i):
        return 2 * ((f // 2 + i) % (NF // 2)) + 1 - c

    def take_direct(b, got, s, r, ms, mr):
        @pl.when(b != f)
        def _():
            remote(got.at[b], got.at[b], s.at[0], r.at[b], fs=b).wait_recv()

        remote(got.at[b], got.at[b], ms.at[b], mr.at[b], tp=z * 2 + 1 - c).start()

    def take_mate(b, got, ms, mr):
        remote(got.at[b], got.at[b], ms.at[b], mr.at[b], tp=z * 2 + 1 - c).wait_recv()

    def wait_mate_sends(got, ms, mr):
        def body(i, carry):
            b = direct_block(i)
            remote(got.at[b], got.at[b], ms.at[b], mr.at[b], tp=z * 2 + 1 - c).wait_send()
            return carry

        lax.fori_loop(0, NF // 2, body, 0)

    along_z(tok_ref, xz, xzs, xzr)

    def send_ids(i, carry):
        remote(idt.at[f], idt.at[f], ids_s.at[i], ids_r.at[f], fs=(f + i) % NF).start()
        return carry

    lax.fori_loop(1, NF, send_ids, 0)

    fr = lax.broadcasted_iota(jnp.int32, (4 * LANES, LANES), 0)
    fc = lax.broadcasted_iota(jnp.int32, (4 * LANES, LANES), 1)
    fold[...] = ((fr // LANES == fc // HS) & (fr % HS == fc % HS)).astype(BF16)
    sr = lax.broadcasted_iota(jnp.int32, (16, K * LANES), 0)
    sc = lax.broadcasted_iota(jnp.int32, (16, K * LANES), 1)
    spread_ids[...] = (sr == sc // LANES).astype(BF16)

    affinity = aff_ref[...]
    weight = ROUTED_SCALE * affinity / jnp.sum(affinity, axis=1, keepdims=True)
    wr = lax.broadcasted_iota(jnp.int32, (K, K * HS), 0)
    wc = lax.broadcasted_iota(jnp.int32, (K, K * HS), 1)
    place = (wr == wc // HS).astype(BF16)
    high = weight.astype(BF16)
    rest = weight - high.astype(F32)
    middle = rest.astype(BF16)
    low = (rest - middle.astype(F32)).astype(BF16)
    wexp[...] = (
        jnp.dot(high, place, preferred_element_type=F32)
        + jnp.dot(middle, place, preferred_element_type=F32)
        + jnp.dot(low, place, preferred_element_type=F32)
    )

    gain = gain_ref[...]
    ws[...] = jnp.zeros_like(ws)
    ws[0:HS, :] = (sgt_ref[...] * gain).astype(BF16)
    ws[HS : 2 * HS, :] = (sut_ref[...] * gain).astype(BF16)
    loads[0].wait()
    loads[1].wait()

    def convert_gate_up(i, carry):
        rows = pl.ds(pl.multiple_of(i * ROWS, ROWS), ROWS)
        wg[rows, :] = (wf[0, rows, :] * gain).astype(BF16)
        wu[rows, :] = (wf[1, rows, :] * gain).astype(BF16)
        return carry

    lax.fori_loop(0, NF, convert_gate_up, 0)

    in_plane(tok_ref, xz, xa, xzs, xzr, xps, xpr)

    wd[EP * NF : EP * NF + EP] = jnp.zeros((EP, HS, DS), BF16)
    wd[EP * NF] = sdt_ref[...].astype(BF16)
    loads[2].wait()

    def convert_down(i, carry):
        rows = pl.ds(pl.multiple_of(i * ROWS, ROWS), ROWS)
        wd[pl.ds(i * EP, EP)] = wf[2, rows, :].reshape(EP, HS, DS).astype(BF16)
        return carry

    lax.fori_loop(0, NF, convert_down, 0)

    def pieces(j, src_of):
        cols = pl.ds(pl.multiple_of(src_of * DS, DS), DS)
        rows = pl.ds(pl.multiple_of(j * ROWS, ROWS), ROWS)
        hid = pl.ds(pl.multiple_of(src_of * HS, HS), HS)
        return (
            (wg.at[rows, :], gs_ref.at[:, cols]),
            (wu.at[rows, :], us_ref.at[:, cols]),
            (wd.at[pl.ds(j * EP, EP)], ds_ref.at[:, hid, :]),
            (ws.at[0:HS, :], sgs_ref.at[:, cols]),
            (ws.at[HS : 2 * HS, :], sus_ref.at[:, cols]),
            (wd.at[EP * NF], sds_ref.at[hid, :]),
        )

    def send_weights(i, which):
        j = (f + i) % NF
        for n, (src, dst) in enumerate(pieces(j, f)):
            if n in which:
                remote(src, dst, w_s.at[n, i], w_r.at[n, f], fs=j).start()

    for n, (src, dst) in enumerate(pieces(f, f)):
        pltpu.make_async_copy(src, dst, own_sem.at[n]).start()

    def partial(b):
        x = xa[b]
        step = 4 * LANES
        for n in range(EH // step):
            part = slice(n * step, (n + 1) * step)
            gsc[:, part] = lax.dot_general(
                x, wg[part, :], NT_DIMS, preferred_element_type=F32
            ).astype(BF16)
            usc[:, part] = lax.dot_general(
                x, wu[part, :], NT_DIMS, preferred_element_type=F32
            ).astype(BF16)
        lane = lax.broadcasted_iota(jnp.int32, (TOK, K * LANES), 1)
        ids = lax.dot_general(idt[b], spread_ids[...], TN_DIMS, preferred_element_type=F32)
        dk[b] = (ids - ((lane % LANES) // HS).astype(F32)).astype(BF16)

        def select(r, carry):
            rows = pl.ds(pl.multiple_of(r * 16, 16), 16)
            at = [dk[b, rows, k * LANES : (k + 1) * LANES] for k in range(K)]
            gate = [jnp.zeros((16, LANES), BF16)] * K
            up = [jnp.zeros((16, LANES), BF16)] * K
            for g in range(GROUPS):
                gv = gsc[rows, g * LANES : (g + 1) * LANES]
                uv = usc[rows, g * LANES : (g + 1) * LANES]
                for k in range(K):
                    hit = at[k] == jnp.asarray(LANES // HS * g, BF16)
                    gate[k] = jnp.where(hit, gv, gate[k])
                    up[k] = jnp.where(hit, uv, up[k])
            for k in range(K):
                tsc[0, rows, k * LANES : (k + 1) * LANES] = gate[k]
                tsc[1, rows, k * LANES : (k + 1) * LANES] = up[k]
            return carry

        lax.fori_loop(0, TOK // 16, select, 0)
        for n in range(2):
            for j in range(2):
                at = (2 * n + j) * LANES
                psend[b, :, at : at + LANES] = jnp.dot(
                    tsc[n, :, j * 4 * LANES : (j + 1) * 4 * LANES],
                    fold[...],
                    preferred_element_type=F32,
                ).astype(BF16)
        shared = lax.dot_general(x, ws[...], NT_DIMS, preferred_element_type=F32)
        xf = x.astype(F32)
        square = jnp.sum(xf * xf, axis=1, keepdims=True)
        first = square.astype(BF16).astype(F32)
        lane = lax.broadcasted_iota(jnp.int32, (TOK, LANES), 1)
        tail = jnp.where(lane < 2 * HS, shared, jnp.where(lane < 3 * HS, first, square - first))
        psend[b, :, 4 * LANES : 5 * LANES] = tail.astype(BF16)

    def send_partial(b):
        @pl.when(b != f)
        def _():
            remote(psend.at[b], precv.at[f], p_s.at[b], p_r.at[f], fs=b).start()

    def take_ids(b):
        @pl.when(b != f)
        def _():
            remote(idt.at[b], idt.at[b], ids_s.at[0], ids_r.at[b], fs=b).wait_recv()

    def first_half(i, carry):
        b = direct_block(i)
        take_ids(b)
        take_direct(b, xa, xps, xpr, xms, xmr)
        partial(b)
        send_partial(b)

        @pl.when(i > 0)
        def _():
            send_weights(i, (0, 1, 2, 3, 4, 5))

        return carry

    lax.fori_loop(0, NF // 2, first_half, 0)

    def second_half(i, carry):
        b = mate_block(i)
        take_ids(b)
        take_mate(b, xa, xms, xmr)
        partial(b)
        send_partial(b)
        return carry

    lax.fori_loop(0, NF // 2, second_half, 0)

    def rest_weights(i, carry):
        send_weights(i, (0, 1, 2, 3, 4, 5))
        return carry

    lax.fori_loop(NF // 2, NF, rest_weights, 0)

    def take_partial(i, carry):
        j = (f + i) % NF
        remote(psend.at[j], precv.at[j], p_s.at[j], p_r.at[j], fs=j).wait_recv()
        return carry

    lax.fori_loop(1, NF, take_partial, 0)

    def finish_hidden(r, carry):
        rows = pl.ds(pl.multiple_of(r * 16, 16), 16)
        total = psend[f, rows, :].astype(F32)
        for i in range(1, NF):
            total = total + precv[(f + i) % NF, rows, :].astype(F32)
        at = 4 * LANES + 2 * HS
        square = total[:, at : at + 1] + total[:, at + HS : at + HS + 1]
        inverse_rms = lax.rsqrt(square * (1.0 / D) + NORM_EPS)
        half = K * HS
        gate = total[:, :half] * inverse_rms
        up = total[:, half : 2 * half] * inverse_rms
        hv[rows, :half] = (silu(gate) * up * wexp[rows, :]).astype(BF16)
        tail = total[:, 4 * LANES :] * inverse_rms
        lane = lax.broadcasted_iota(jnp.int32, (16, LANES), 1)
        shared = silu(tail) * pltpu.roll(tail, LANES - HS, 1)
        hv[rows, half : half + LANES] = jnp.where(lane < HS, shared, 0.0).astype(BF16)
        return carry

    lax.fori_loop(0, TOK // 16, finish_hidden, 0)

    along_z(hv, hz, hzs, hzr)
    in_plane(hv, hz, ha, hzs, hzr, hps, hpr)

    def down(b):
        for j in range(2):
            tsc[0, :, j * 4 * LANES : (j + 1) * 4 * LANES] = lax.dot_general(
                ha[b, :, j * LANES : (j + 1) * LANES],
                fold[...],
                NT_DIMS,
                preferred_element_type=F32,
            ).astype(BF16)

        def scatter(r, carry):
            rows = pl.ds(pl.multiple_of(r * 16, 16), 16)
            at = [dk[b, rows, k * LANES : (k + 1) * LANES] for k in range(K)]
            hid = [tsc[0, rows, k * LANES : (k + 1) * LANES] for k in range(K)]
            for g in range(GROUPS):
                a = jnp.zeros((16, LANES), BF16)
                for k in range(K):
                    a = jnp.where(at[k] == jnp.asarray(LANES // HS * g, BF16), hid[k], a)
                asc[rows, g * LANES : (g + 1) * LANES] = a
            asc[rows, EH : EH + LANES] = ha[b, rows, 2 * LANES : 3 * LANES]
            return carry

        lax.fori_loop(0, TOK // 16, scatter, 0)
        osend[b] = jnp.dot(
            asc[...], wd[...].reshape(EH + LANES, DS), preferred_element_type=F32
        ).astype(BF16)

    def send_out(b):
        @pl.when(b != f)
        def _():
            remote(osend.at[b], orecv.at[f], o_s.at[b], o_r.at[f], fs=b).start()

    def down_first(i, carry):
        b = direct_block(i)
        take_direct(b, ha, hps, hpr, hms, hmr)
        down(b)
        send_out(b)
        return carry

    def down_second(i, carry):
        b = mate_block(i)
        take_mate(b, ha, hms, hmr)
        down(b)
        send_out(b)
        return carry

    lax.fori_loop(0, NF // 2, down_first, 0)
    lax.fori_loop(0, NF // 2, down_second, 0)

    def take_out(i, carry):
        j = (f + i) % NF
        remote(osend.at[j], orecv.at[j], o_s.at[j], o_r.at[j], fs=j).wait_recv()
        return carry

    lax.fori_loop(1, NF, take_out, 0)

    def finish(r, carry):
        rows = pl.ds(pl.multiple_of(r * 16, 16), 16)
        total = osend[f, rows, :].astype(F32)
        for i in range(1, NF):
            total = total + orecv[(f + i) % NF, rows, :].astype(F32)
        mixed_ref[rows, :] = total.astype(BF16)
        return carry

    lax.fori_loop(0, TOK // 16, finish, 0)

    for n, (src, dst) in enumerate(pieces(f, f)):
        pltpu.make_async_copy(src, dst, own_sem.at[n]).wait()
    wait_spread_sends(tok_ref, xz, xa, xzs, xzr, xps, xpr)
    wait_spread_sends(hv, hz, ha, hzs, hzr, hps, hpr)
    wait_mate_sends(xa, xms, xmr)
    wait_mate_sends(ha, hms, hmr)

    def drain(i, carry):
        j = (f + i) % NF
        remote(idt.at[f], idt.at[f], ids_s.at[i], ids_r.at[f], fs=j).wait_send()
        remote(psend.at[j], precv.at[f], p_s.at[j], p_r.at[f], fs=j).wait_send()
        remote(osend.at[j], orecv.at[f], o_s.at[j], o_r.at[f], fs=j).wait_send()
        for n, (src, dst) in enumerate(pieces(j, f)):
            remote(src, dst, w_s.at[n, i], w_r.at[n, f], fs=j).wait_send()
        for n, (src, dst) in enumerate(pieces(f, j)):
            remote(src, dst, w_s.at[n, i], w_r.at[n, j], fs=j).wait_recv()
        return carry

    lax.fori_loop(1, NF, drain, 0)


def solution(mesh):
    NF, NT = mesh.shape["fs"], mesh.shape["tp"]

    def body(tokens, ids, affinity, gain, gt, ut, dt, sgt, sut, sdt):
        TOK, DS = tokens.shape
        E, HS, _ = gt.shape
        EP = E // NF
        EH = E * HS
        NZ = NT // 2
        D = DS * NF
        H = HS * NT
        C = 5 * LANES
        hbm = pl.BlockSpec(memory_space=pl.ANY)
        vmem = pl.BlockSpec(memory_space=pltpu.VMEM)
        dma = pltpu.SemaphoreType.DMA
        outs = pl.pallas_call(
            functools.partial(kernel, NF, NT, D),
            out_shape=(
                jax.ShapeDtypeStruct((TOK, DS), BF16),
                jax.ShapeDtypeStruct((EP * HS, D), BF16),
                jax.ShapeDtypeStruct((EP * HS, D), BF16),
                jax.ShapeDtypeStruct((EP, H, DS), BF16),
                jax.ShapeDtypeStruct((HS, D), BF16),
                jax.ShapeDtypeStruct((HS, D), BF16),
                jax.ShapeDtypeStruct((H, DS), BF16),
            ),
            in_specs=[vmem] * 4 + [hbm] * 3 + [vmem] * 3,
            out_specs=[vmem] + [hbm] * 6,
            scratch_shapes=[
                pltpu.VMEM((3, EH, DS), F32),
                pltpu.VMEM((EH, DS), BF16),
                pltpu.VMEM((EH, DS), BF16),
                pltpu.VMEM((E + EP, HS, DS), BF16),
                pltpu.VMEM((LANES, DS), BF16),
                pltpu.VMEM((4 * LANES, LANES), BF16),
                pltpu.VMEM((16, K * LANES), BF16),
                pltpu.VMEM((TOK, K * HS), F32),
                pltpu.VMEM((NF, 16, TOK), BF16),
                pltpu.VMEM((NZ, TOK, DS), BF16),
                pltpu.VMEM((NF, TOK, DS), BF16),
                pltpu.VMEM((TOK, 3 * LANES), BF16),
                pltpu.VMEM((NZ, TOK, 3 * LANES), BF16),
                pltpu.VMEM((NF, TOK, 3 * LANES), BF16),
                pltpu.VMEM((NF, TOK, K * LANES), BF16),
                pltpu.VMEM((TOK, EH), BF16),
                pltpu.VMEM((TOK, EH), BF16),
                pltpu.VMEM((2, TOK, K * LANES), BF16),
                pltpu.VMEM((TOK, EH + LANES), BF16),
                pltpu.VMEM((NF, TOK, C), BF16),
                pltpu.VMEM((NF, TOK, C), BF16),
                pltpu.VMEM((NF, TOK, DS), BF16),
                pltpu.VMEM((NF, TOK, DS), BF16),
                dma((3,)),
                dma((6,)),
                dma((NF,)),
                dma((NF,)),
                *[dma((NZ,)), dma((NZ,)), dma((NZ,)), dma((NF,)), dma((NF,)), dma((NF,))] * 2,
                *[dma((NF,))] * 4,
                dma((6, NF)),
                dma((6, NF)),
            ],
            compiler_params=pltpu.CompilerParams(
                collective_id=0,
                has_side_effects=True,
                vmem_limit_bytes=60 * 1024 * 1024,
            ),
        )(
            tokens, ids, affinity, gain.reshape(1, DS),
            gt.reshape(EH, DS), ut.reshape(EH, DS), dt.reshape(EH, DS), sgt, sut, sdt,
        )
        mixed, gs, us, ds, sgs, sus, sds = outs
        return mixed, gs.reshape(EP, HS, D), us.reshape(EP, HS, D), ds, sgs, sus, sds

    return jax.shard_map(
        body,
        mesh=mesh,
        in_specs=(
            P("fs", "tp"),
            P("fs", None),
            P("fs", None),
            P("fs"),
            P(None, "tp", "fs"),
            P(None, "tp", "fs"),
            P(None, "fs", "tp"),
            P("tp", "fs"),
            P("tp", "fs"),
            P("fs", "tp"),
        ),
        out_specs=(
            P("fs", "tp"),
            P("fs", "tp", None),
            P("fs", "tp", None),
            P("fs", None, "tp"),
            P("tp", None),
            P("tp", None),
            P(None, "tp"),
        ),
        check_vma=False,
    )
```

```python
import functools
import math

import jax
import jax.numpy as jnp
from jax import lax
from jax.experimental import pallas as pl
from jax.experimental.pallas import tpu as pltpu
from jax.sharding import PartitionSpec as P

K = 8
NORM_EPS = 1e-06
ROUTED_SCALE = 2.5
LANES = 128
WIDE = 256
F32 = jnp.float32
BF16 = jnp.bfloat16
NT_DIMS = (((1,), (1,)), ((), ()))
TN_DIMS = (((0,), (0,)), ((), ()))


def silu(v):
    return v / (1.0 + jnp.exp(-v))


def kernel(
    NF,
    NT,
    D,
    tok_ref,
    ids_ref,
    aff_ref,
    gain_ref,
    gt_ref,
    ut_ref,
    dt_ref,
    sgt_ref,
    sut_ref,
    sdt_ref,
    mixed_ref,
    gs_ref,
    us_ref,
    ds_ref,
    sgs_ref,
    sus_ref,
    sds_ref,
    wf,
    wg,
    wu,
    wd,
    ws,
    fold,
    spread_ids,
    wexp,
    idt,
    xz,
    xa,
    sq,
    hv,
    hz,
    ha,
    dk,
    gsc,
    usc,
    tsc,
    asc,
    tail_asc,
    psend,
    qa,
    qb,
    sa,
    sb,
    pa,
    pb,
    ptot,
    osend,
    orecv,
    load_sem,
    own_sem,
    ids_s,
    ids_r,
    xzs,
    xzr,
    xps,
    xpr,
    xms,
    xmr,
    hzs,
    hzr,
    hps,
    hpr,
    hms,
    hmr,
    p_s,
    p_r,
    p2_s,
    p2_r,
    o_s,
    o_r,
    w_s,
    w_r,
    sq_s,
    sq_r,
):
    f = lax.axis_index("fs")
    t = lax.axis_index("tp")
    z, c = t // 2, t % 2
    NZ = NT // 2
    TOK, DS = tok_ref.shape
    HS = sgt_ref.shape[0]
    EH = wg.shape[0]
    EP = EH // HS // NF
    GROUPS = EH // WIDE
    ROWS = EP * HS

    loads = []
    for i, r in enumerate((gt_ref, ut_ref, dt_ref)):
        load = pltpu.make_async_copy(r, wf.at[i], load_sem.at[i])
        load.start()
        loads.append(load)

    bar = pltpu.get_barrier_semaphore()

    def greet_plane(i, carry):
        at = (f * 2 + c + i) % (2 * NF)
        pl.semaphore_signal(
            bar, 1, device_id={"fs": at // 2, "tp": z * 2 + at % 2},
            device_id_type=pl.DeviceIdType.MESH,
        )
        return carry

    def greet_column(i, carry):
        pl.semaphore_signal(
            bar, 1, device_id={"tp": ((z + i) % NZ) * 2 + c},
            device_id_type=pl.DeviceIdType.MESH,
        )
        return carry

    lax.fori_loop(1, 2 * NF, greet_plane, 0)
    lax.fori_loop(1, NZ, greet_column, 0)

    idt[f] = jnp.concatenate([ids_ref[...].astype(F32), jnp.zeros((16 - K, TOK), F32)], axis=0).astype(BF16)

    pl.semaphore_wait(bar, 2 * NF - 1 + NZ - 1)

    def remote(src, dst, s, r, **where):
        return pltpu.make_async_remote_copy(
            src_ref=src, dst_ref=dst, send_sem=s, recv_sem=r,
            device_id=where, device_id_type=pl.DeviceIdType.MESH,
        )

    steps = [i for d in range(1, NZ // 2 + 1) for i in dict.fromkeys((d, NZ - d))]

    def along_z(src, stage, s, r):
        for i in steps:
            remote(src, stage.at[z], s.at[i], r.at[z], tp=((z + i) % NZ) * 2 + c).start()

    def in_plane(src, stage, got, zs, zr, s, r, beside=None):
        for n, i in enumerate([0] + [(NZ - i) for i in steps]):
            zz = (z + i) % NZ
            if i:
                remote(src, stage.at[zz], zs.at[i], zr.at[zz], tp=zz * 2 + c).wait_recv()
            part = stage.at[zz] if i else src
            to = zz * 2 + c

            @pl.when(to == f)
            def _():
                got[f] = part[...]

            @pl.when(to != f)
            def _():
                remote(part, got.at[f], s.at[i], r.at[f], fs=to, tp=z * 2 + f % 2).start()

            if beside is not None:
                beside(n)

    def wait_spread_sends(src, stage, got, zs, zr, s, r):
        for i in range(NZ):
            zz = (z + i) % NZ
            to = zz * 2 + c
            if i:
                remote(src, stage.at[z], zs.at[i], zr.at[z], tp=zz * 2 + c).wait_send()

            @pl.when(to != f)
            def _():
                remote(src, got.at[f], s.at[i], r.at[f], fs=to, tp=z * 2 + f % 2).wait_send()

    def direct_block(i):
        return 2 * ((f // 2 + i) % (NF // 2)) + c

    def take_direct(b, got, s, r, ms, mr):
        @pl.when(b != f)
        def _():
            remote(got.at[b], got.at[b], s.at[0], r.at[b], fs=b).wait_recv()

        remote(got.at[b], got.at[b], ms.at[b], mr.at[b], tp=z * 2 + 1 - c).start()

    def take_mate(b, got, ms, mr):
        remote(got.at[b], got.at[b], ms.at[b], mr.at[b], tp=z * 2 + 1 - c).wait_recv()

    def wait_mate_sends(got, ms, mr):
        def body(i, carry):
            b = direct_block(i)
            remote(got.at[b], got.at[b], ms.at[b], mr.at[b], tp=z * 2 + 1 - c).wait_send()
            return carry

        lax.fori_loop(0, NF // 2, body, 0)

    along_z(tok_ref, xz, xzs, xzr)

    def send_ids(i, carry):
        remote(idt.at[f], idt.at[f], ids_s.at[i], ids_r.at[f], fs=(f + i) % NF).start()
        return carry

    lax.fori_loop(1, NF, send_ids, 0)

    fr = lax.broadcasted_iota(jnp.int32, (4 * WIDE, LANES), 0)
    fc = lax.broadcasted_iota(jnp.int32, (4 * WIDE, LANES), 1)
    fold[...] = ((fr // WIDE == fc // HS) & (fr % HS == fc % HS)).astype(BF16)
    sr = lax.broadcasted_iota(jnp.int32, (16, K * WIDE), 0)
    sc = lax.broadcasted_iota(jnp.int32, (16, K * WIDE), 1)
    spread_ids[...] = (sr == sc // WIDE).astype(BF16)

    affinity = aff_ref[...]
    weight = ROUTED_SCALE * affinity / jnp.sum(affinity, axis=0, keepdims=True)
    wr = lax.broadcasted_iota(jnp.int32, (K, K * HS), 0)
    wc = lax.broadcasted_iota(jnp.int32, (K, K * HS), 1)
    place = (wr == wc // HS).astype(BF16)
    high = weight.astype(BF16)
    rest = weight - high.astype(F32)
    middle = rest.astype(BF16)
    low = (rest - middle.astype(F32)).astype(BF16)
    wexp[...] = (
        lax.dot_general(high, place, TN_DIMS, preferred_element_type=F32)
        + lax.dot_general(middle, place, TN_DIMS, preferred_element_type=F32)
        + lax.dot_general(low, place, TN_DIMS, preferred_element_type=F32)
    )

    gain = gain_ref[...]
    ws[...] = jnp.zeros_like(ws)
    ws[0:HS, :DS] = (sgt_ref[...] * gain).astype(BF16)
    ws[HS : 2 * HS, :DS] = (sut_ref[...] * gain).astype(BF16)
    ws[2 * HS :, DS:] = ws[0 : 2 * HS, :DS]
    loads[0].wait()
    loads[1].wait()

    def convert_gate_up(i, carry):
        rows = pl.ds(pl.multiple_of(i * ROWS, ROWS), ROWS)
        wg[rows, :] = (wf[0, rows, :] * gain).astype(BF16)
        wu[rows, :] = (wf[1, rows, :] * gain).astype(BF16)
        return carry

    lax.fori_loop(0, NF, convert_gate_up, 0)

    shared_down = sdt_ref[...].astype(BF16)
    for i in range(LANES // HS):
        wd[EP * NF + i] = shared_down
    loads[2].wait()

    def convert_down(i, carry):
        rows = pl.ds(pl.multiple_of(i * ROWS, ROWS), ROWS)
        wd[pl.ds(i * EP, EP)] = wf[2, rows, :].reshape(EP, HS, DS).astype(BF16)
        return carry

    lax.fori_loop(0, NF, convert_down, 0)

    def pieces(j, src_of):
        cols = pl.ds(pl.multiple_of(src_of * DS, DS), DS)
        rows = pl.ds(pl.multiple_of(j * ROWS, ROWS), ROWS)
        hid = pl.ds(pl.multiple_of(src_of * HS, HS), HS)
        return (
            (wg.at[rows, :], gs_ref.at[:, cols]),
            (wu.at[rows, :], us_ref.at[:, cols]),
            (wd.at[pl.ds(j * EP, EP)], ds_ref.at[:, hid, :]),
            (ws.at[0:HS, 0:DS], sgs_ref.at[:, cols]),
            (ws.at[HS : 2 * HS, 0:DS], sus_ref.at[:, cols]),
            (wd.at[EP * NF], sds_ref.at[hid, :]),
        )

    def send_weights(which, first, last):
        def body(i, carry):
            j = (f + i) % NF
            for n, (src, dst) in enumerate(pieces(j, f)):
                if n in which:
                    remote(src, dst, w_s.at[n, i], w_r.at[n, f], fs=j).start()
            return carry

        lax.fori_loop(first, last, body, 0)

    def pair_of(p):
        def block(i):
            late = i // (NF // 2)
            return 2 * ((f // 2 + i) % (NF // 2)) + (c + late) % 2

        return block(2 * p), block(2 * p + 1)

    def take_ids(b):
        @pl.when(b != f)
        def _():
            remote(idt.at[b], idt.at[b], ids_s.at[0], ids_r.at[b], fs=b).wait_recv()

    def compare(p):
        lane = lax.broadcasted_iota(jnp.int32, (TOK, WIDE), 1)
        quarter = (lane // HS).astype(F32)
        for u, b in enumerate(pair_of(p)):
            take_ids(b)
            ids = lax.dot_general(idt[b], spread_ids[...], TN_DIMS, preferred_element_type=F32)
            for k in range(K):
                dk[p, k, u * TOK : (u + 1) * TOK] = (
                    ids[:, k * WIDE : (k + 1) * WIDE] - quarter
                ).astype(BF16)

    def compare_pairs(n):
        def body(p, carry):
            compare(p)
            return carry

        lax.fori_loop(n * NF // (2 * NZ), (n + 1) * NF // (2 * NZ), body, 0)

    send_weights((0,), 1, NF)
    in_plane(tok_ref, xz, xa, xzs, xzr, xps, xpr, compare_pairs)
    send_weights((3, 4, 5), 1, NF)

    square = jnp.square(tok_ref[...].astype(F32))
    for i in range(1, NZ):
        square = square + jnp.square(xz[(z + i) % NZ].astype(F32))
    sq[0] = jnp.broadcast_to(jnp.sum(square, axis=1, keepdims=True), (TOK, LANES))
    swap = remote(sq.at[0], sq.at[1], sq_s, sq_r, tp=z * 2 + 1 - c)
    swap.start()


    for n, (src, dst) in enumerate(pieces(f, f)):
        pltpu.make_async_copy(src, dst, own_sem.at[n]).start()

    def partial(p):
        b0, b1 = pair_of(p)
        x0, x1 = xa[b0], xa[b1]
        x = jnp.concatenate([x0, x1], axis=0)
        step = 4 * LANES
        for n in range(EH // step):
            part = slice(n * step, (n + 1) * step)
            for w, to in ((wg, gsc), (wu, usc)):
                y = lax.dot_general(x, w[part, :], NT_DIMS, preferred_element_type=F32).astype(BF16)
                for q in range(2):
                    to[2 * n + q] = y[:, q * WIDE : (q + 1) * WIDE]

        def select(r, carry):
            rows = pl.ds(pl.multiple_of(r * 16, 16), 16)
            for k in range(K):
                at = dk[p, k, rows]
                gate = jnp.zeros((16, WIDE), BF16)
                up = jnp.zeros((16, WIDE), BF16)
                for g in range(GROUPS):
                    hit = at == jnp.asarray(WIDE // HS * g, BF16)
                    gate = jnp.where(hit, gsc[g, rows], gate)
                    up = jnp.where(hit, usc[g, rows], up)
                tsc[0, k, rows] = gate
                tsc[1, k, rows] = up
            return carry

        lax.fori_loop(0, 2 * TOK // 16, select, 0)
        for n in range(2):
            for j in range(2):
                at = (2 * n + j) * LANES
                y = jnp.dot(
                    jnp.concatenate([tsc[n, 4 * j + q] for q in range(4)], axis=1),
                    fold[...],
                    preferred_element_type=F32,
                ).astype(BF16)
                psend[b0, :TOK, at : at + LANES] = y[:TOK]
                psend[b1, :TOK, at : at + LANES] = y[TOK:]
        half = TOK // 2
        halves = jnp.concatenate(
            [
                jnp.concatenate([x0[:half], x1[:half]], axis=0),
                jnp.concatenate([x0[half:], x1[half:]], axis=0),
            ],
            axis=1,
        )
        y = lax.dot_general(halves, ws[...], NT_DIMS, preferred_element_type=F32).astype(BF16)
        for q in range(4):
            at = slice(q * LANES, (q + 1) * LANES)
            psend[b0, TOK:, at] = y[16 * q : 16 * q + 16]
            psend[b1, TOK:, at] = y[half + 16 * q : half + 16 * q + 16]

    NX = math.isqrt(NF)
    y, x = f // NX, f % NX
    HALF = (TOK + 16) // 2
    upper, lower = pl.ds(0, HALF), pl.ds(HALF, HALF)

    def upper_copy(b):
        to = y * NX + b % NX
        return remote(
            psend.at[b, upper], qa.at[x, b // NX], p_s.at[0, b], p_r.at[0, x * NX + b // NX], fs=to
        )

    def lower_copy(b):
        to = b // NX * NX + x
        return remote(
            psend.at[b, lower], qb.at[y, b % NX], p_s.at[1, b], p_r.at[1, y * NX + b % NX], fs=to
        )

    def send_partial(b):
        @pl.when(b % NX != x)
        def _():
            upper_copy(b).start()

        @pl.when(b // NX != y)
        def _():
            lower_copy(b).start()

    def add_up(dst, terms):
        for r in range(3):
            at = slice(HALF // 3 * r, HALF // 3 * (r + 1))
            total = terms[0][at].astype(F32)
            for term in terms[1:]:
                total = total + term[at].astype(F32)
            dst[at] = total.astype(dst.dtype)

    def partial_step(p, carry):
        b0, b1 = pair_of(p)
        @pl.when(p < NF // 4)
        def _():
            take_direct(b0, xa, xps, xpr, xms, xmr)
            take_direct(b1, xa, xps, xpr, xms, xmr)

        @pl.when(p >= NF // 4)
        def _():
            take_mate(b0, xa, xms, xmr)
            take_mate(b1, xa, xms, xmr)

        partial(p)
        send_partial(b0)
        send_partial(b1)
        return carry

    lax.fori_loop(0, NF // 2, partial_step, 0)
    swap.wait_recv()

    def second_upper(yb):
        return remote(sa.at[yb], pa.at[y], p2_s.at[0, yb], p2_r.at[0, y], fs=yb * NX + x)

    def second_lower(xb):
        return remote(sb.at[xb], pb.at[x], p2_s.at[1, xb], p2_r.at[1, x], fs=y * NX + xb)

    for i in list(range(1, NX)) + [0]:
        yb, xb = (y + i) % NX, (x + i) % NX
        for j in range(1, NX):
            xs, ys = (x + j) % NX, (y + j) % NX
            remote(
                psend.at[0, upper], qa.at[xs, yb], p_s.at[0, 0], p_r.at[0, xs * NX + yb], fs=f
            ).wait_recv()
            remote(
                psend.at[0, lower], qb.at[ys, xb], p_s.at[1, 0], p_r.at[1, ys * NX + xb], fs=f
            ).wait_recv()
        add_up(
            sa.at[yb],
            [psend.at[yb * NX + x, upper]] + [qa.at[(x + j) % NX, yb] for j in range(1, NX)],
        )
        add_up(
            sb.at[xb],
            [psend.at[y * NX + xb, lower]] + [qb.at[(y + j) % NX, xb] for j in range(1, NX)],
        )
        if i:
            second_upper(yb).start()
            second_lower(xb).start()
    pass
    for i in range(1, NX):
        ys, xs = (y + i) % NX, (x + i) % NX
        remote(sa.at[0], pa.at[ys], p2_s.at[0, 0], p2_r.at[0, ys], fs=f).wait_recv()
        remote(sb.at[0], pb.at[xs], p2_s.at[1, 0], p2_r.at[1, xs], fs=f).wait_recv()
    add_up(ptot.at[upper], [sa.at[y]] + [pa.at[(y + i) % NX] for i in range(1, NX)])
    add_up(ptot.at[lower], [sb.at[x]] + [pb.at[(x + i) % NX] for i in range(1, NX)])

    def summed(mine, got, rows):
        total = mine[f, rows, :].astype(F32)
        for i in range(1, NF):
            total = total + got[(f + i) % NF, rows, :].astype(F32)
        return total

    half = K * HS
    inverse_rms = lax.rsqrt((sq[0] + sq[1]) * (1.0 / D) + NORM_EPS)
    for r in range(TOK // 16):
        rows = slice(16 * r, 16 * r + 16)
        total = ptot[rows, :]
        inv = jnp.concatenate([inverse_rms[rows]] * (half // LANES), axis=1)
        hidden = silu(total[:, :half] * inv) * (total[:, half:] * inv) * wexp[rows, :]
        hv[rows, :] = hidden.astype(BF16)
    lane = lax.broadcasted_iota(jnp.int32, (16, LANES), 1)
    total = ptot[TOK:, :]
    low, high = jnp.zeros((16, LANES), F32), jnp.zeros((16, LANES), F32)
    for q in range(4):
        inv = jnp.where(
            lane < 2 * HS,
            inverse_rms[16 * q : 16 * q + 16],
            inverse_rms[16 * q + TOK // 2 : 16 * q + TOK // 2 + 16],
        )
        pre = total[:, q * LANES : (q + 1) * LANES] * inv
        shared = silu(pre) * pltpu.roll(pre, LANES - HS, 1)
        here = lane // HS == q
        first = pltpu.roll(shared, HS * q, 1) if q else shared
        second = pltpu.roll(shared, (HS * q + 2 * HS) % LANES, 1) if q != 2 else shared
        low = jnp.where(here, first, low)
        high = jnp.where(here, second, high)
    hv[TOK:, :LANES] = low.astype(BF16)
    hv[TOK:, LANES:] = high.astype(BF16)

    along_z(hv, hz, hzs, hzr)
    send_weights((1,), 1, NF)
    in_plane(hv, hz, ha, hzs, hzr, hps, hpr)
    send_weights((2,), 1, NF)

    pass

    def down(p):
        b0, b1 = pair_of(p)
        for j in range(2):
            at = slice(j * LANES, (j + 1) * LANES)
            y = lax.dot_general(
                jnp.concatenate([ha[b0, :TOK, at], ha[b1, :TOK, at]], axis=0),
                fold[...],
                NT_DIMS,
                preferred_element_type=F32,
            ).astype(BF16)
            for q in range(4):
                tsc[0, 4 * j + q] = y[:, q * WIDE : (q + 1) * WIDE]

        def scatter(r, carry):
            rows = pl.ds(pl.multiple_of(r * 16, 16), 16)
            at = [dk[p, k, rows] for k in range(K)]
            hid = [tsc[0, k, rows] for k in range(K)]
            for g in range(GROUPS):
                a = jnp.zeros((16, WIDE), BF16)
                for k in range(K):
                    a = jnp.where(at[k] == jnp.asarray(WIDE // HS * g, BF16), hid[k], a)
                asc[g, rows] = a
            b = b0 + (r // (TOK // 16)) * (b1 - b0)
            s = r % (TOK // 16)
            tail = ha[b, TOK:, pl.ds(pl.multiple_of(s // 4 * LANES, LANES), LANES)]
            lane = lax.broadcasted_iota(jnp.int32, (16, LANES), 1)
            tail_asc[rows] = jnp.where(lane // HS == s % 4, tail.astype(F32), 0.0).astype(BF16)
            return carry

        lax.fori_loop(0, 2 * TOK // 16, scatter, 0)
        y = jnp.dot(
            jnp.concatenate([asc[g] for g in range(GROUPS)] + [tail_asc[...]], axis=1),
            wd[...].reshape(EH + LANES, DS),
            preferred_element_type=F32,
        ).astype(BF16)
        osend[b0] = y[:TOK]
        osend[b1] = y[TOK:]

    def send_out(b):
        @pl.when(b != f)
        def _():
            remote(osend.at[b], orecv.at[f], o_s.at[b], o_r.at[f], fs=b).start()

    def down_step(p, carry):
        b0, b1 = pair_of(p)

        @pl.when(p < NF // 4)
        def _():
            take_direct(b0, ha, hps, hpr, hms, hmr)
            take_direct(b1, ha, hps, hpr, hms, hmr)

        @pl.when(p >= NF // 4)
        def _():
            take_mate(b0, ha, hms, hmr)
            take_mate(b1, ha, hms, hmr)

        down(p)
        send_out(b0)
        send_out(b1)
        return carry

    lax.fori_loop(0, NF // 2, down_step, 0)

    def take_out(i, carry):
        j = (f + i) % NF
        remote(osend.at[j], orecv.at[j], o_s.at[j], o_r.at[j], fs=j).wait_recv()
        return carry

    lax.fori_loop(1, NF, take_out, 0)

    def finish(r, carry):
        rows = pl.ds(pl.multiple_of(r * 16, 16), 16)
        mixed_ref[rows, :] = summed(osend, orecv, rows).astype(BF16)
        return carry

    lax.fori_loop(0, TOK // 16, finish, 0)

    swap.wait_send()
    for n, (src, dst) in enumerate(pieces(f, f)):
        pltpu.make_async_copy(src, dst, own_sem.at[n]).wait()
    wait_spread_sends(tok_ref, xz, xa, xzs, xzr, xps, xpr)
    wait_spread_sends(hv, hz, ha, hzs, hzr, hps, hpr)
    wait_mate_sends(xa, xms, xmr)
    wait_mate_sends(ha, hms, hmr)

    def drain(i, carry):
        j = (f + i) % NF
        remote(idt.at[f], idt.at[f], ids_s.at[i], ids_r.at[f], fs=j).wait_send()
        remote(osend.at[j], orecv.at[f], o_s.at[j], o_r.at[f], fs=j).wait_send()
        for n, (src, dst) in enumerate(pieces(j, f)):
            remote(src, dst, w_s.at[n, i], w_r.at[n, f], fs=j).wait_send()
        for n, (src, dst) in enumerate(pieces(f, j)):
            remote(src, dst, w_s.at[n, i], w_r.at[n, j], fs=j).wait_recv()
        return carry

    lax.fori_loop(1, NF, drain, 0)

    def drain_partial(b, carry):
        @pl.when(b % NX != x)
        def _():
            upper_copy(b).wait_send()

        @pl.when(b // NX != y)
        def _():
            lower_copy(b).wait_send()

        return carry

    lax.fori_loop(0, NF, drain_partial, 0)
    for i in range(1, NX):
        second_upper((y + i) % NX).wait_send()
        second_lower((x + i) % NX).wait_send()


def place(n, *refs):
    src, dst, held, s_in, s_out = refs[:n], refs[n : 2 * n], refs[2 * n : 3 * n], refs[-2], refs[-1]
    parts = []
    for a, b, h in zip(src, dst, held):
        rows = a.shape[0]
        cuts = 4 if rows % 64 == 0 and a.shape[-1] * rows > 1 << 18 else 1
        for i in range(cuts):
            at = pl.ds(rows // cuts * i, rows // cuts)
            parts.append((a.at[at], b.at[at], h.at[at]))
    for i, (a, b, h) in enumerate(parts):
        pltpu.make_async_copy(a, h, s_in.at[i]).start()
    for i, (a, b, h) in enumerate(parts):
        pltpu.make_async_copy(a, h, s_in.at[i]).wait()
        pltpu.make_async_copy(h, b, s_out.at[i]).start()
    for i, (a, b, h) in enumerate(parts):
        pltpu.make_async_copy(h, b, s_out.at[i]).wait()


def solution(mesh):
    NF, NT = mesh.shape["fs"], mesh.shape["tp"]

    def body(tokens, ids, affinity, gain, gt, ut, dt, sgt, sut, sdt):
        TOK, DS = tokens.shape
        E, HS, _ = gt.shape
        EP = E // NF
        EH = E * HS
        NZ = NT // 2
        NX = math.isqrt(NF)
        D = DS * NF
        H = HS * NT
        hbm = pl.BlockSpec(memory_space=pl.ANY)
        vmem = pl.BlockSpec(memory_space=pltpu.VMEM)
        dma = pltpu.SemaphoreType.DMA
        outs = pl.pallas_call(
            functools.partial(kernel, NF, NT, D),
            out_shape=(
                jax.ShapeDtypeStruct((TOK, DS), BF16),
                jax.ShapeDtypeStruct((EP * HS, D), BF16),
                jax.ShapeDtypeStruct((EP * HS, D), BF16),
                jax.ShapeDtypeStruct((EP, H, DS), BF16),
                jax.ShapeDtypeStruct((HS, D), BF16),
                jax.ShapeDtypeStruct((HS, D), BF16),
                jax.ShapeDtypeStruct((H, DS), BF16),
            ),
            in_specs=[vmem] * 4 + [hbm] * 3 + [vmem] * 3,
            out_specs=[vmem] + [hbm] * 6,
            scratch_shapes=[
                pltpu.VMEM((3, EH, DS), F32),
                pltpu.VMEM((EH, DS), BF16),
                pltpu.VMEM((EH, DS), BF16),
                pltpu.VMEM((E + LANES // HS, HS, DS), BF16),
                pltpu.VMEM((LANES, 2 * DS), BF16),
                pltpu.VMEM((4 * WIDE, LANES), BF16),
                pltpu.VMEM((16, K * WIDE), BF16),
                pltpu.VMEM((TOK, K * HS), F32),
                pltpu.VMEM((NF, 16, TOK), BF16),
                pltpu.VMEM((NZ, TOK, DS), BF16),
                pltpu.VMEM((NF, TOK, DS), BF16),
                pltpu.VMEM((2, TOK, LANES), F32),
                pltpu.VMEM((TOK + 16, K * HS), BF16),
                pltpu.VMEM((NZ, TOK + 16, K * HS), BF16),
                pltpu.VMEM((NF, TOK + 16, K * HS), BF16),
                pltpu.VMEM((NF // 2, K, 2 * TOK, WIDE), BF16),
                pltpu.VMEM((EH // WIDE, 2 * TOK, WIDE), BF16),
                pltpu.VMEM((EH // WIDE, 2 * TOK, WIDE), BF16),
                pltpu.VMEM((2, K, 2 * TOK, WIDE), BF16),
                pltpu.VMEM((EH // WIDE, 2 * TOK, WIDE), BF16),
                pltpu.VMEM((2 * TOK, LANES), BF16),
                pltpu.VMEM((NF, TOK + 16, 2 * K * HS), BF16),
                *[pltpu.VMEM((NX, NX, (TOK + 16) // 2, 2 * K * HS), BF16)] * 2,
                *[pltpu.VMEM((NX, (TOK + 16) // 2, 2 * K * HS), BF16)] * 4,
                pltpu.VMEM((TOK + 16, 2 * K * HS), F32),
                pltpu.VMEM((NF, TOK, DS), BF16),
                pltpu.VMEM((NF, TOK, DS), BF16),
                dma((3,)),
                dma((6,)),
                dma((NF,)),
                dma((NF,)),
                *[dma((NZ,)), dma((NZ,)), dma((NZ,)), dma((NF,)), dma((NF,)), dma((NF,))] * 2,
                *[dma((2, NF))] * 2,
                *[dma((2, NX))] * 2,
                *[dma((NF,))] * 2,
                dma((6, NF)),
                dma((6, NF)),
                dma,
                dma,
            ],
            compiler_params=pltpu.CompilerParams(
                collective_id=0,
                has_side_effects=True,
                vmem_limit_bytes=60 * 1024 * 1024,
            ),
        )(
            tokens, ids.T, affinity.T, gain.reshape(1, DS),
            gt.reshape(EH, DS), ut.reshape(EH, DS), dt.reshape(EH, DS), sgt, sut, sdt,
        )
        n = len(outs)
        outs = (*outs[:3], outs[3].reshape(EP * H, DS), *outs[4:])
        shapes = [jax.ShapeDtypeStruct(a.shape, a.dtype) for a in outs]
        outs = pl.pallas_call(
            functools.partial(place, n),
            out_shape=shapes,
            in_specs=[hbm] * n,
            out_specs=[hbm] * n,
            scratch_shapes=[pltpu.VMEM(a.shape, a.dtype) for a in shapes] + [dma((4 * n,))] * 2,
            compiler_params=pltpu.CompilerParams(vmem_limit_bytes=60 * 1024 * 1024),
        )(*outs)
        mixed, gs, us, ds, sgs, sus, sds = outs
        ds = ds.reshape(EP, H, DS)
        return mixed, gs.reshape(EP, HS, D), us.reshape(EP, HS, D), ds, sgs, sus, sds

    return jax.shard_map(
        body,
        mesh=mesh,
        in_specs=(
            P("fs", "tp"),
            P("fs", None),
            P("fs", None),
            P("fs"),
            P(None, "tp", "fs"),
            P(None, "tp", "fs"),
            P(None, "fs", "tp"),
            P("tp", "fs"),
            P("tp", "fs"),
            P("fs", "tp"),
        ),
        out_specs=(
            P("fs", "tp"),
            P("fs", "tp", None),
            P("fs", "tp", None),
            P("fs", None, "tp"),
            P("tp", None),
            P("tp", None),
            P(None, "tp"),
        ),
        check_vma=False,
    )
```

```python
import functools
import math

import jax
import jax.numpy as jnp
from jax import lax
from jax.experimental import pallas as pl
from jax.experimental.pallas import tpu as pltpu
from jax.sharding import PartitionSpec as P

K = 8
NORM_EPS = 1e-06
ROUTED_SCALE = 2.5
LANES = 128
F32 = jnp.float32
BF16 = jnp.bfloat16
NT_DIMS = (((1,), (1,)), ((), ()))
TN_DIMS = (((0,), (0,)), ((), ()))


def silu(v):
    return v / (1.0 + jnp.exp(-v))


def kernel(
    NF,
    NT,
    D,
    tok_ref,
    ids_ref,
    aff_ref,
    gain_ref,
    gt_ref,
    ut_ref,
    dt_ref,
    sgt_ref,
    sut_ref,
    sdt_ref,
    mixed_ref,
    gs_ref,
    us_ref,
    ds_ref,
    sgs_ref,
    sus_ref,
    sds_ref,
    wf,
    wg,
    wu,
    wd,
    ws,
    wgp,
    wup,
    wdp,
    spread_ids,
    wexp,
    idt,
    xz,
    xa,
    sq,
    hv,
    hz,
    ha,
    choice,
    expert,
    pre,
    asc,
    tail_asc,
    psend,
    qa,
    qb,
    sa,
    sb,
    pa,
    pb,
    ptot,
    osend,
    orecv,
    load_sem,
    own_sem,
    ids_s,
    ids_r,
    xzs,
    xzr,
    xps,
    xpr,
    xms,
    xmr,
    hzs,
    hzr,
    hps,
    hpr,
    hms,
    hmr,
    p_s,
    p_r,
    p2_s,
    p2_r,
    o_s,
    o_r,
    w_s,
    w_r,
    sq_s,
    sq_r,
):
    f = lax.axis_index("fs")
    t = lax.axis_index("tp")
    z, c = t // 2, t % 2
    NZ = NT // 2
    TOK, DS = tok_ref.shape
    HS = sgt_ref.shape[0]
    EH = wg.shape[0]
    EP = EH // HS // NF
    TILES = EH // LANES
    E = EP * NF
    ROWS = EP * HS

    loads = []
    for i, r in enumerate((gt_ref, ut_ref, dt_ref)):
        for q in range(DS // LANES):
            load = pltpu.make_async_copy(
                r.at[:, q * LANES : (q + 1) * LANES], wf.at[2 * i + q], load_sem.at[2 * i + q]
            )
            load.start()
            loads.append(load)

    bar = pltpu.get_barrier_semaphore()

    def greet_plane(i, carry):
        at = (f * 2 + c + i) % (2 * NF)
        pl.semaphore_signal(
            bar, 1, device_id={"fs": at // 2, "tp": z * 2 + at % 2},
            device_id_type=pl.DeviceIdType.MESH,
        )
        return carry

    def greet_column(i, carry):
        pl.semaphore_signal(
            bar, 1, device_id={"tp": ((z + i) % NZ) * 2 + c},
            device_id_type=pl.DeviceIdType.MESH,
        )
        return carry

    lax.fori_loop(1, 2 * NF, greet_plane, 0)
    lax.fori_loop(1, NZ, greet_column, 0)

    idt[f] = jnp.concatenate([ids_ref[...].astype(F32), jnp.zeros((16 - K, TOK), F32)], axis=0).astype(BF16)

    pl.semaphore_wait(bar, 2 * NF - 1 + NZ - 1)

    def remote(src, dst, s, r, **where):
        return pltpu.make_async_remote_copy(
            src_ref=src, dst_ref=dst, send_sem=s, recv_sem=r,
            device_id=where, device_id_type=pl.DeviceIdType.MESH,
        )

    steps = [i for d in range(1, NZ // 2 + 1) for i in dict.fromkeys((d, NZ - d))]

    def along_z(src, stage, s, r):
        for i in steps:
            remote(src, stage.at[z], s.at[i], r.at[z], tp=((z + i) % NZ) * 2 + c).start()

    def in_plane(src, stage, got, zs, zr, s, r, beside=None):
        for n, i in enumerate([0] + [(NZ - i) for i in steps]):
            zz = (z + i) % NZ
            if i:
                remote(src, stage.at[zz], zs.at[i], zr.at[zz], tp=zz * 2 + c).wait_recv()
            part = stage.at[zz] if i else src
            to = zz * 2 + c

            @pl.when(to == f)
            def _():
                got[f] = part[...]

            @pl.when(to != f)
            def _():
                remote(part, got.at[f], s.at[i], r.at[f], fs=to, tp=z * 2 + f % 2).start()

            if beside is not None:
                beside(n)

    def wait_spread_sends(src, stage, got, zs, zr, s, r):
        for i in range(NZ):
            zz = (z + i) % NZ
            to = zz * 2 + c
            if i:
                remote(src, stage.at[z], zs.at[i], zr.at[z], tp=zz * 2 + c).wait_send()

            @pl.when(to != f)
            def _():
                remote(src, got.at[f], s.at[i], r.at[f], fs=to, tp=z * 2 + f % 2).wait_send()

    def direct_block(i):
        return 2 * ((f // 2 + i) % (NF // 2)) + c

    def take_direct(b, got, s, r, ms, mr):
        @pl.when(b != f)
        def _():
            remote(got.at[b], got.at[b], s.at[0], r.at[b], fs=b).wait_recv()

        remote(got.at[b], got.at[b], ms.at[b], mr.at[b], tp=z * 2 + 1 - c).start()

    def take_mate(b, got, ms, mr):
        remote(got.at[b], got.at[b], ms.at[b], mr.at[b], tp=z * 2 + 1 - c).wait_recv()

    def wait_mate_sends(got, ms, mr):
        def body(i, carry):
            b = direct_block(i)
            remote(got.at[b], got.at[b], ms.at[b], mr.at[b], tp=z * 2 + 1 - c).wait_send()
            return carry

        lax.fori_loop(0, NF // 2, body, 0)

    along_z(tok_ref, xz, xzs, xzr)

    def send_ids(i, carry):
        remote(idt.at[f], idt.at[f], ids_s.at[i], ids_r.at[f], fs=(f + i) % NF).start()
        return carry

    lax.fori_loop(1, NF, send_ids, 0)

    sr = lax.broadcasted_iota(jnp.int32, (16, K * LANES), 0)
    sc = lax.broadcasted_iota(jnp.int32, (16, K * LANES), 1)
    spread_ids[:, : K * LANES] = (sr == sc // LANES).astype(BF16)
    spread_ids[:, K * LANES :] = (sr[:, :LANES] == sc[:, :LANES] % K).astype(BF16)

    affinity = aff_ref[...]
    weight = ROUTED_SCALE * affinity / jnp.sum(affinity, axis=0, keepdims=True)
    wr = lax.broadcasted_iota(jnp.int32, (K, K * HS), 0)
    wc = lax.broadcasted_iota(jnp.int32, (K, K * HS), 1)
    place = (wr == wc % K).astype(BF16)
    high = weight.astype(BF16)
    rest = weight - high.astype(F32)
    middle = rest.astype(BF16)
    low = (rest - middle.astype(F32)).astype(BF16)
    wexp[...] = (
        lax.dot_general(high, place, TN_DIMS, preferred_element_type=F32)
        + lax.dot_general(middle, place, TN_DIMS, preferred_element_type=F32)
        + lax.dot_general(low, place, TN_DIMS, preferred_element_type=F32)
    )

    gain = gain_ref[...]
    ws[...] = jnp.zeros_like(ws)
    ws[0:HS, :DS] = (sgt_ref[...] * gain).astype(BF16)
    ws[HS : 2 * HS, :DS] = (sut_ref[...] * gain).astype(BF16)
    ws[2 * HS :, DS:] = ws[0 : 2 * HS, :DS]
    for load in loads[:4]:
        load.wait()
    halves = [slice(q * LANES, (q + 1) * LANES) for q in range(DS // LANES)]

    def convert_gate_up(i, carry):
        rows = pl.ds(pl.multiple_of(i * ROWS, ROWS), ROWS)
        for q, at in enumerate(halves):
            wg[rows, at] = (wf[q, rows, :] * gain[:, at]).astype(BF16)
            wu[rows, at] = (wf[2 + q, rows, :] * gain[:, at]).astype(BF16)
        return carry

    lax.fori_loop(0, NF, convert_gate_up, 0)

    def reorder_gate_up(h, carry):
        rows = pl.ds(pl.multiple_of(h * E, E), E)
        for q, at in enumerate(halves):
            wgp[rows, at] = (wf[q, pl.ds(h, E, stride=HS), :] * gain[:, at]).astype(BF16)
            wup[rows, at] = (wf[2 + q, pl.ds(h, E, stride=HS), :] * gain[:, at]).astype(BF16)
        return carry


    shared_down = sdt_ref[...].astype(BF16)
    wd[E] = shared_down
    for load in loads[4:]:
        load.wait()

    def convert_down(i, carry):
        rows = pl.ds(pl.multiple_of(i * ROWS, ROWS), ROWS)
        for q, at in enumerate(halves):
            wd[pl.ds(i * EP, EP), :, at] = wf[4 + q, rows, :].reshape(EP, HS, LANES).astype(BF16)
        return carry

    lax.fori_loop(0, NF, convert_down, 0)
    for i in range(LANES // HS):
        wdp[EH + i * HS : EH + (i + 1) * HS, :] = shared_down

    def reorder_down(h, carry):
        rows = pl.ds(pl.multiple_of(h * E, E), E)
        for q, at in enumerate(halves):
            wdp[rows, at] = wf[4 + q, pl.ds(h, E, stride=HS), :].astype(BF16)
        return carry


    def pieces(j, src_of):
        cols = pl.ds(pl.multiple_of(src_of * DS, DS), DS)
        rows = pl.ds(pl.multiple_of(j * ROWS, ROWS), ROWS)
        hid = pl.ds(pl.multiple_of(src_of * HS, HS), HS)
        return (
            (wg.at[rows, :], gs_ref.at[:, cols]),
            (wu.at[rows, :], us_ref.at[:, cols]),
            (wd.at[pl.ds(j * EP, EP)], ds_ref.at[:, hid, :]),
            (ws.at[0:HS, 0:DS], sgs_ref.at[:, cols]),
            (ws.at[HS : 2 * HS, 0:DS], sus_ref.at[:, cols]),
            (wd.at[EP * NF], sds_ref.at[hid, :]),
        )

    def send_weights(which, first, last):
        def body(i, carry):
            j = (f + i + c * (NF - 2 * i)) % NF
            for n, (src, dst) in enumerate(pieces(j, f)):
                if n in which:
                    remote(src, dst, w_s.at[n, i], w_r.at[n, f], fs=j).start()
            return carry

        lax.fori_loop(first, last, body, 0)

    def pair_of(p):
        def block(i):
            late = i // (NF // 2)
            return 2 * ((f // 2 + i) % (NF // 2)) + (c + late) % 2

        return block(2 * p), block(2 * p + 1)

    def take_ids(b):
        @pl.when(b != f)
        def _():
            remote(idt.at[b], idt.at[b], ids_s.at[0], ids_r.at[b], fs=b).wait_recv()

    def compare(p):
        lane = lax.broadcasted_iota(jnp.int32, (TOK, LANES), 1)
        for b in pair_of(p):
            take_ids(b)
            ids = lax.dot_general(
                idt[b], spread_ids[...], TN_DIMS, preferred_element_type=F32
            ).astype(jnp.int32)
            choice[b] = (lane // K) % (LANES // E) * E + ids[:, K * LANES :]
            at = jnp.full((TOK, LANES), -1, jnp.int32)
            for k in range(K):
                at = jnp.where(ids[:, k * LANES : (k + 1) * LANES] == lane % E, lane // E * K + k, at)
            expert[b] = at

    def compare_pairs(n):
        def body(p, carry):
            compare(p)
            return carry

        lax.fori_loop(n * NF // (2 * NZ), (n + 1) * NF // (2 * NZ), body, 0)
        lax.fori_loop(n * HS // NZ, (n + 1) * HS // NZ, reorder_gate_up, 0)
        lax.fori_loop(n * HS // NZ, (n + 1) * HS // NZ, reorder_down, 0)

    send_weights((0,), 1, NF)
    in_plane(tok_ref, xz, xa, xzs, xzr, xps, xpr, compare_pairs)
    send_weights((3, 4, 5), 1, NF)

    square = jnp.square(tok_ref[...].astype(F32))
    for i in range(1, NZ):
        square = square + jnp.square(xz[(z + i) % NZ].astype(F32))
    sq[0] = jnp.broadcast_to(jnp.sum(square, axis=1, keepdims=True), (TOK, LANES))
    swap = remote(sq.at[0], sq.at[1], sq_s, sq_r, tp=z * 2 + 1 - c)
    swap.start()


    for n, (src, dst) in enumerate(pieces(f, f)):
        pltpu.make_async_copy(src, dst, own_sem.at[n]).start()

    def partial(p):
        b0, b1 = pair_of(p)
        x0, x1 = xa[b0], xa[b1]
        x = jnp.concatenate([x0, x1], axis=0)
        step = 4 * LANES
        for n in range(EH // step):
            part = slice(n * step, (n + 1) * step)
            for i, w in enumerate((wgp, wup)):
                y = lax.dot_general(x, w[part, :], NT_DIMS, preferred_element_type=F32)
                for q in range(4):
                    pre[i * TILES + 4 * n + q] = y[:, q * LANES : (q + 1) * LANES]
        per = LANES // (K * (LANES // E))

        lane = lax.broadcasted_iota(jnp.int32, (16, LANES), 1)
        group = lane // (LANES // per)

        def select(m, carry):
            for u in range(4):
                r = 4 * m + u
                rows = pl.ds(pl.multiple_of(r * 16, 16), 16)
                b = b0 + r // (TOK // 16) * (b1 - b0)
                here = pl.ds(pl.multiple_of(r % (TOK // 16) * 16, 16), 16)
                at = choice[b, here]
                for o in range(2 * TILES // per):
                    total = jnp.take_along_axis(pre[o * per, rows], at, axis=1)
                    for j in range(1, per):
                        value = jnp.take_along_axis(pre[o * per + j, rows], at, axis=1)
                        total = jnp.where(group == j, value, total)
                    psend[b, here, o * LANES : (o + 1) * LANES] = total.astype(BF16)
            return carry

        lax.fori_loop(0, 2 * TOK // 64, select, 0)
        half = TOK // 2
        two = jnp.concatenate(
            [
                jnp.concatenate([x0[:half], x1[:half]], axis=0),
                jnp.concatenate([x0[half:], x1[half:]], axis=0),
            ],
            axis=1,
        )
        y = lax.dot_general(two, ws[...], NT_DIMS, preferred_element_type=F32).astype(BF16)
        for q in range(4):
            at = slice(q * LANES, (q + 1) * LANES)
            psend[b0, TOK:, at] = y[16 * q : 16 * q + 16]
            psend[b1, TOK:, at] = y[half + 16 * q : half + 16 * q + 16]

    NX = math.isqrt(NF)
    y, x = f // NX, f % NX
    HALF = (TOK + 16) // 2
    upper, lower = pl.ds(0, HALF), pl.ds(HALF, HALF)

    def upper_copy(b):
        to = y * NX + b % NX
        return remote(
            psend.at[b, upper], qa.at[x, b // NX], p_s.at[0, b], p_r.at[0, x * NX + b // NX], fs=to
        )

    def lower_copy(b):
        to = b // NX * NX + x
        return remote(
            psend.at[b, lower], qb.at[y, b % NX], p_s.at[1, b], p_r.at[1, y * NX + b % NX], fs=to
        )

    def send_partial(b):
        @pl.when(b % NX != x)
        def _():
            upper_copy(b).start()

        @pl.when(b // NX != y)
        def _():
            lower_copy(b).start()

    def add_up(dst, terms):
        for r in range(3):
            at = slice(HALF // 3 * r, HALF // 3 * (r + 1))
            total = terms[0][at].astype(F32)
            for term in terms[1:]:
                total = total + term[at].astype(F32)
            dst[at] = total.astype(dst.dtype)

    def partial_step(p, carry):
        b0, b1 = pair_of(p)
        @pl.when(p < NF // 4)
        def _():
            take_direct(b0, xa, xps, xpr, xms, xmr)
            take_direct(b1, xa, xps, xpr, xms, xmr)

        @pl.when(p >= NF // 4)
        def _():
            take_mate(b0, xa, xms, xmr)
            take_mate(b1, xa, xms, xmr)

        partial(p)
        send_partial(b0)
        send_partial(b1)
        return carry

    lax.fori_loop(0, NF // 2, partial_step, 0)
    swap.wait_recv()

    def second_upper(yb):
        return remote(sa.at[yb], pa.at[y], p2_s.at[0, yb], p2_r.at[0, y], fs=yb * NX + x)

    def second_lower(xb):
        return remote(sb.at[xb], pb.at[x], p2_s.at[1, xb], p2_r.at[1, x], fs=y * NX + xb)

    for i in list(range(1, NX)) + [0]:
        yb, xb = (y + i) % NX, (x + i) % NX
        for j in range(1, NX):
            xs, ys = (x + j) % NX, (y + j) % NX
            remote(
                psend.at[0, upper], qa.at[xs, yb], p_s.at[0, 0], p_r.at[0, xs * NX + yb], fs=f
            ).wait_recv()
            remote(
                psend.at[0, lower], qb.at[ys, xb], p_s.at[1, 0], p_r.at[1, ys * NX + xb], fs=f
            ).wait_recv()
        add_up(
            sa.at[yb],
            [psend.at[yb * NX + x, upper]] + [qa.at[(x + j) % NX, yb] for j in range(1, NX)],
        )
        add_up(
            sb.at[xb],
            [psend.at[y * NX + xb, lower]] + [qb.at[(y + j) % NX, xb] for j in range(1, NX)],
        )
        if i:
            second_upper(yb).start()
            second_lower(xb).start()
    pass
    for i in range(1, NX):
        ys, xs = (y + i) % NX, (x + i) % NX
        remote(sa.at[0], pa.at[ys], p2_s.at[0, 0], p2_r.at[0, ys], fs=f).wait_recv()
        remote(sb.at[0], pb.at[xs], p2_s.at[1, 0], p2_r.at[1, xs], fs=f).wait_recv()
    add_up(ptot.at[upper], [sa.at[y]] + [pa.at[(y + i) % NX] for i in range(1, NX)])
    add_up(ptot.at[lower], [sb.at[x]] + [pb.at[(x + i) % NX] for i in range(1, NX)])

    def summed(mine, got, rows):
        total = mine[f, rows, :].astype(F32)
        for i in range(1, NF):
            total = total + got[(f + i) % NF, rows, :].astype(F32)
        return total

    half = K * HS
    inverse_rms = lax.rsqrt((sq[0] + sq[1]) * (1.0 / D) + NORM_EPS)
    for r in range(TOK // 16):
        rows = slice(16 * r, 16 * r + 16)
        total = ptot[rows, :]
        inv = jnp.concatenate([inverse_rms[rows]] * (half // LANES), axis=1)
        hidden = silu(total[:, :half] * inv) * (total[:, half:] * inv) * wexp[rows, :]
        hv[rows, :] = hidden.astype(BF16)
    lane = lax.broadcasted_iota(jnp.int32, (16, LANES), 1)
    total = ptot[TOK:, :]
    low, high = jnp.zeros((16, LANES), F32), jnp.zeros((16, LANES), F32)
    for q in range(4):
        inv = jnp.where(
            lane < 2 * HS,
            inverse_rms[16 * q : 16 * q + 16],
            inverse_rms[16 * q + TOK // 2 : 16 * q + TOK // 2 + 16],
        )
        pre = total[:, q * LANES : (q + 1) * LANES] * inv
        shared = silu(pre) * pltpu.roll(pre, LANES - HS, 1)
        here = lane // HS == q
        first = pltpu.roll(shared, HS * q, 1) if q else shared
        second = pltpu.roll(shared, (HS * q + 2 * HS) % LANES, 1) if q != 2 else shared
        low = jnp.where(here, first, low)
        high = jnp.where(here, second, high)
    hv[TOK:, :LANES] = low.astype(BF16)
    hv[TOK:, LANES:] = high.astype(BF16)

    along_z(hv, hz, hzs, hzr)
    send_weights((1,), 1, NF)
    send_weights((2,), 1, NF)
    in_plane(hv, hz, ha, hzs, hzr, hps, hpr)

    pass

    def down(p):
        b0, b1 = pair_of(p)
        per = LANES // (K * (LANES // E))

        lane = lax.broadcasted_iota(jnp.int32, (16, LANES), 1)

        def scatter(m, carry):
            for u in range(4):
                r = 4 * m + u
                rows = pl.ds(pl.multiple_of(r * 16, 16), 16)
                b = b0 + r // (TOK // 16) * (b1 - b0)
                s = r % (TOK // 16)
                here = pl.ds(pl.multiple_of(s * 16, 16), 16)
                at = expert[b, here]
                chosen = at >= 0
                at = jnp.maximum(at, 0)
                for o in range(TILES // per):
                    hidden = ha[b, here, o * LANES : (o + 1) * LANES].astype(F32)
                    for j in range(per):
                        value = jnp.take_along_axis(hidden, at + j * (LANES // per), axis=1)
                        asc[o * per + j, rows] = jnp.where(chosen, value, 0.0).astype(BF16)
                tail = ha[b, TOK:, pl.ds(pl.multiple_of(s // 4 * LANES, LANES), LANES)]
                tail_asc[rows] = jnp.where(lane // HS == s % 4, tail.astype(F32), 0.0).astype(BF16)
            return carry

        lax.fori_loop(0, 2 * TOK // 64, scatter, 0)
        y = jnp.dot(
            jnp.concatenate([asc[g] for g in range(TILES)] + [tail_asc[...]], axis=1),
            wdp[...],
            preferred_element_type=F32,
        ).astype(BF16)
        osend[b0] = y[:TOK]
        osend[b1] = y[TOK:]

    def send_out(b):
        @pl.when(b != f)
        def _():
            remote(osend.at[b], orecv.at[f], o_s.at[b], o_r.at[f], fs=b).start()

    def down_step(p, carry):
        b0, b1 = pair_of(p)

        @pl.when(p < NF // 4)
        def _():
            take_direct(b0, ha, hps, hpr, hms, hmr)
            take_direct(b1, ha, hps, hpr, hms, hmr)

        @pl.when(p >= NF // 4)
        def _():
            take_mate(b0, ha, hms, hmr)
            take_mate(b1, ha, hms, hmr)

        down(p)
        send_out(b0)
        send_out(b1)
        return carry

    lax.fori_loop(0, NF // 2, down_step, 0)

    def take_out(i, carry):
        j = (f + i) % NF
        remote(osend.at[j], orecv.at[j], o_s.at[j], o_r.at[j], fs=j).wait_recv()
        return carry

    lax.fori_loop(1, NF, take_out, 0)

    def finish(r, carry):
        rows = pl.ds(pl.multiple_of(r * 16, 16), 16)
        mixed_ref[rows, :] = summed(osend, orecv, rows).astype(BF16)
        return carry

    lax.fori_loop(0, TOK // 16, finish, 0)

    swap.wait_send()
    for n, (src, dst) in enumerate(pieces(f, f)):
        pltpu.make_async_copy(src, dst, own_sem.at[n]).wait()
    wait_spread_sends(tok_ref, xz, xa, xzs, xzr, xps, xpr)
    wait_spread_sends(hv, hz, ha, hzs, hzr, hps, hpr)
    wait_mate_sends(xa, xms, xmr)
    wait_mate_sends(ha, hms, hmr)

    def drain(i, carry):
        j = (f + i) % NF
        remote(idt.at[f], idt.at[f], ids_s.at[i], ids_r.at[f], fs=j).wait_send()
        remote(osend.at[j], orecv.at[f], o_s.at[j], o_r.at[f], fs=j).wait_send()
        for n, (src, dst) in enumerate(pieces(j, f)):
            remote(src, dst, w_s.at[n, i], w_r.at[n, f], fs=j).wait_send()
        for n, (src, dst) in enumerate(pieces(f, j)):
            remote(src, dst, w_s.at[n, i], w_r.at[n, j], fs=j).wait_recv()
        return carry

    lax.fori_loop(1, NF, drain, 0)

    def drain_partial(b, carry):
        @pl.when(b % NX != x)
        def _():
            upper_copy(b).wait_send()

        @pl.when(b // NX != y)
        def _():
            lower_copy(b).wait_send()

        return carry

    lax.fori_loop(0, NF, drain_partial, 0)
    for i in range(1, NX):
        second_upper((y + i) % NX).wait_send()
        second_lower((x + i) % NX).wait_send()


def place(n, *refs):
    src, dst, held, s_in, s_out = refs[:n], refs[n : 2 * n], refs[2 * n : 3 * n], refs[-2], refs[-1]
    parts = []
    for a, b, h in zip(src, dst, held):
        rows = a.shape[0]
        cuts = 4 if rows % 64 == 0 and a.shape[-1] * rows > 1 << 18 else 1
        for i in range(cuts):
            at = pl.ds(rows // cuts * i, rows // cuts)
            parts.append((a.at[at], b.at[at], h.at[at]))
    for i, (a, b, h) in enumerate(parts):
        pltpu.make_async_copy(a, h, s_in.at[i]).start()
    for i, (a, b, h) in enumerate(parts):
        pltpu.make_async_copy(a, h, s_in.at[i]).wait()
        pltpu.make_async_copy(h, b, s_out.at[i]).start()
    for i, (a, b, h) in enumerate(parts):
        pltpu.make_async_copy(h, b, s_out.at[i]).wait()


def solution(mesh):
    NF, NT = mesh.shape["fs"], mesh.shape["tp"]

    def body(tokens, ids, affinity, gain, gt, ut, dt, sgt, sut, sdt):
        TOK, DS = tokens.shape
        E, HS, _ = gt.shape
        EP = E // NF
        EH = E * HS
        NZ = NT // 2
        NX = math.isqrt(NF)
        D = DS * NF
        H = HS * NT
        hbm = pl.BlockSpec(memory_space=pl.ANY)
        vmem = pl.BlockSpec(memory_space=pltpu.VMEM)
        dma = pltpu.SemaphoreType.DMA
        outs = pl.pallas_call(
            functools.partial(kernel, NF, NT, D),
            out_shape=(
                jax.ShapeDtypeStruct((TOK, DS), BF16),
                jax.ShapeDtypeStruct((EP * HS, D), BF16),
                jax.ShapeDtypeStruct((EP * HS, D), BF16),
                jax.ShapeDtypeStruct((EP, H, DS), BF16),
                jax.ShapeDtypeStruct((HS, D), BF16),
                jax.ShapeDtypeStruct((HS, D), BF16),
                jax.ShapeDtypeStruct((H, DS), BF16),
            ),
            in_specs=[vmem] * 4 + [hbm] * 3 + [vmem] * 3,
            out_specs=[vmem] + [hbm] * 6,
            scratch_shapes=[
                pltpu.VMEM((6, EH, LANES), F32),
                pltpu.VMEM((EH, DS), BF16),
                pltpu.VMEM((EH, DS), BF16),
                pltpu.VMEM((E + 1, HS, DS), BF16),
                pltpu.VMEM((LANES, 2 * DS), BF16),
                pltpu.VMEM((EH, DS), BF16),
                pltpu.VMEM((EH, DS), BF16),
                pltpu.VMEM((EH + LANES, DS), BF16),
                pltpu.VMEM((16, (K + 1) * LANES), BF16),
                pltpu.VMEM((TOK, K * HS), F32),
                pltpu.VMEM((NF, 16, TOK), BF16),
                pltpu.VMEM((NZ, TOK, DS), BF16),
                pltpu.VMEM((NF, TOK, DS), BF16),
                pltpu.VMEM((2, TOK, LANES), F32),
                pltpu.VMEM((TOK + 16, K * HS), BF16),
                pltpu.VMEM((NZ, TOK + 16, K * HS), BF16),
                pltpu.VMEM((NF, TOK + 16, K * HS), BF16),
                pltpu.VMEM((NF, TOK, LANES), jnp.int32),
                pltpu.VMEM((NF, TOK, LANES), jnp.int32),
                pltpu.VMEM((2 * EH // LANES, 2 * TOK, LANES), F32),
                pltpu.VMEM((EH // LANES, 2 * TOK, LANES), BF16),
                pltpu.VMEM((2 * TOK, LANES), BF16),
                pltpu.VMEM((NF, TOK + 16, 2 * K * HS), BF16),
                *[pltpu.VMEM((NX, NX, (TOK + 16) // 2, 2 * K * HS), BF16)] * 2,
                *[pltpu.VMEM((NX, (TOK + 16) // 2, 2 * K * HS), BF16)] * 4,
                pltpu.VMEM((TOK + 16, 2 * K * HS), F32),
                pltpu.VMEM((NF, TOK, DS), BF16),
                pltpu.VMEM((NF, TOK, DS), BF16),
                dma((6,)),
                dma((6,)),
                dma((NF,)),
                dma((NF,)),
                *[dma((NZ,)), dma((NZ,)), dma((NZ,)), dma((NF,)), dma((NF,)), dma((NF,))] * 2,
                *[dma((2, NF))] * 2,
                *[dma((2, NX))] * 2,
                *[dma((NF,))] * 2,
                dma((6, NF)),
                dma((6, NF)),
                dma,
                dma,
            ],
            compiler_params=pltpu.CompilerParams(
                collective_id=0,
                has_side_effects=True,
                vmem_limit_bytes=60 * 1024 * 1024,
            ),
        )(
            tokens, ids.T, affinity.T, gain.reshape(1, DS),
            gt.reshape(EH, DS), ut.reshape(EH, DS), dt.reshape(EH, DS), sgt, sut, sdt,
        )
        n = len(outs)
        outs = (*outs[:3], outs[3].reshape(EP * H, DS), *outs[4:])
        shapes = [jax.ShapeDtypeStruct(a.shape, a.dtype) for a in outs]
        outs = pl.pallas_call(
            functools.partial(place, n),
            out_shape=shapes,
            in_specs=[hbm] * n,
            out_specs=[hbm] * n,
            scratch_shapes=[pltpu.VMEM(a.shape, a.dtype) for a in shapes] + [dma((4 * n,))] * 2,
            compiler_params=pltpu.CompilerParams(vmem_limit_bytes=60 * 1024 * 1024),
        )(*outs)
        mixed, gs, us, ds, sgs, sus, sds = outs
        ds = ds.reshape(EP, H, DS)
        return mixed, gs.reshape(EP, HS, D), us.reshape(EP, HS, D), ds, sgs, sus, sds

    return jax.shard_map(
        body,
        mesh=mesh,
        in_specs=(
            P("fs", "tp"),
            P("fs", None),
            P("fs", None),
            P("fs"),
            P(None, "tp", "fs"),
            P(None, "tp", "fs"),
            P(None, "fs", "tp"),
            P("tp", "fs"),
            P("tp", "fs"),
            P("fs", "tp"),
        ),
        out_specs=(
            P("fs", "tp"),
            P("fs", "tp", None),
            P("fs", "tp", None),
            P("fs", None, "tp"),
            P("tp", None),
            P("tp", None),
            P(None, "tp"),
        ),
        check_vma=False,
    )
```

```python
import functools
import math

import jax
import jax.numpy as jnp
from jax import lax
from jax.experimental import pallas as pl
from jax.experimental.pallas import tpu as pltpu
from jax.sharding import PartitionSpec as P

K = 8
NORM_EPS = 1e-06
ROUTED_SCALE = 2.5
LANES = 128
F32 = jnp.float32
BF16 = jnp.bfloat16
NT_DIMS = (((1,), (1,)), ((), ()))
TN_DIMS = (((0,), (0,)), ((), ()))


def silu(v):
    return v / (1.0 + jnp.exp(-v))


def kernel(
    NF,
    NT,
    D,
    tok_ref,
    ids_ref,
    aff_ref,
    gain_ref,
    gt_ref,
    ut_ref,
    dt_ref,
    sgt_ref,
    sut_ref,
    sdt_ref,
    mixed_ref,
    gs_ref,
    us_ref,
    ds_ref,
    sgs_ref,
    sus_ref,
    sds_ref,
    wf,
    wg,
    wu,
    wd,
    ws,
    wgp,
    wup,
    wdp,
    spread_ids,
    wexp,
    idt,
    xz,
    xa,
    sq,
    hv,
    hz,
    ha,
    choice,
    expert,
    pre,
    asc,
    tail_asc,
    psend,
    qa,
    qb,
    sa,
    sb,
    pa,
    pb,
    ptot,
    osend,
    orecv,
    load_sem,
    own_sem,
    ids_s,
    ids_r,
    xzs,
    xzr,
    xps,
    xpr,
    xms,
    xmr,
    hzs,
    hzr,
    hps,
    hpr,
    hms,
    hmr,
    p_s,
    p_r,
    p2_s,
    p2_r,
    o_s,
    o_r,
    w_s,
    w_r,
    sq_s,
    sq_r,
):
    f = lax.axis_index("fs")
    t = lax.axis_index("tp")
    z, c = t // 2, t % 2
    NZ = NT // 2
    TOK, DS = tok_ref.shape
    HS = sgt_ref.shape[0]
    EH = wg.shape[0]
    EP = EH // HS // NF
    TILES = EH // LANES
    E = EP * NF
    ROWS = EP * HS

    loads = []
    for i, r in enumerate((gt_ref, ut_ref, dt_ref)):
        for q in range(DS // LANES):
            load = pltpu.make_async_copy(
                r.at[:, q * LANES : (q + 1) * LANES], wf.at[2 * i + q], load_sem.at[2 * i + q]
            )
            load.start()
            loads.append(load)

    bar = pltpu.get_barrier_semaphore()

    def greet_plane(i, carry):
        at = (f * 2 + c + i) % (2 * NF)
        pl.semaphore_signal(
            bar, 1, device_id={"fs": at // 2, "tp": z * 2 + at % 2},
            device_id_type=pl.DeviceIdType.MESH,
        )
        return carry

    def greet_column(i, carry):
        pl.semaphore_signal(
            bar, 1, device_id={"tp": ((z + i) % NZ) * 2 + c},
            device_id_type=pl.DeviceIdType.MESH,
        )
        return carry

    lax.fori_loop(1, 2 * NF, greet_plane, 0)
    lax.fori_loop(1, NZ, greet_column, 0)

    idt[f] = jnp.concatenate([ids_ref[...].astype(F32), jnp.zeros((16 - K, TOK), F32)], axis=0).astype(BF16)

    sr = lax.broadcasted_iota(jnp.int32, (16, K * LANES), 0)
    sc = lax.broadcasted_iota(jnp.int32, (16, K * LANES), 1)
    spread_ids[:, : K * LANES] = (sr == sc // LANES).astype(BF16)
    spread_ids[:, K * LANES :] = (sr[:, :LANES] == sc[:, :LANES] % K).astype(BF16)

    affinity = aff_ref[...]
    weight = ROUTED_SCALE * affinity / jnp.sum(affinity, axis=0, keepdims=True)
    wr = lax.broadcasted_iota(jnp.int32, (K, K * HS), 0)
    wc = lax.broadcasted_iota(jnp.int32, (K, K * HS), 1)
    place = (wr == wc % K).astype(BF16)
    high = weight.astype(BF16)
    rest = weight - high.astype(F32)
    middle = rest.astype(BF16)
    low = (rest - middle.astype(F32)).astype(BF16)
    wexp[...] = (
        lax.dot_general(high, place, TN_DIMS, preferred_element_type=F32)
        + lax.dot_general(middle, place, TN_DIMS, preferred_element_type=F32)
        + lax.dot_general(low, place, TN_DIMS, preferred_element_type=F32)
    )

    gain = gain_ref[...]
    ws[...] = jnp.zeros_like(ws)
    ws[0:HS, :DS] = (sgt_ref[...] * gain).astype(BF16)
    ws[HS : 2 * HS, :DS] = (sut_ref[...] * gain).astype(BF16)
    ws[2 * HS :, DS:] = ws[0 : 2 * HS, :DS]
    pl.semaphore_wait(bar, 2 * NF - 1 + NZ - 1)

    def remote(src, dst, s, r, **where):
        return pltpu.make_async_remote_copy(
            src_ref=src, dst_ref=dst, send_sem=s, recv_sem=r,
            device_id=where, device_id_type=pl.DeviceIdType.MESH,
        )

    steps = [i for d in range(1, NZ // 2 + 1) for i in dict.fromkeys((d, NZ - d))]

    def along_z(src, stage, s, r):
        for i in steps:
            remote(src, stage.at[z], s.at[i], r.at[z], tp=((z + i) % NZ) * 2 + c).start()

    def in_plane(src, stage, got, zs, zr, s, r, beside=None):
        for n, i in enumerate([0] + [(NZ - i) for i in steps]):
            zz = (z + i) % NZ
            if i:
                remote(src, stage.at[zz], zs.at[i], zr.at[zz], tp=zz * 2 + c).wait_recv()
            part = stage.at[zz] if i else src
            to = zz * 2 + c

            @pl.when(to == f)
            def _():
                got[f] = part[...]

            @pl.when(to != f)
            def _():
                remote(part, got.at[f], s.at[i], r.at[f], fs=to, tp=z * 2 + f % 2).start()

            if beside is not None:
                beside(n)

    def wait_spread_sends(src, stage, got, zs, zr, s, r):
        for i in range(NZ):
            zz = (z + i) % NZ
            to = zz * 2 + c
            if i:
                remote(src, stage.at[z], zs.at[i], zr.at[z], tp=zz * 2 + c).wait_send()

            @pl.when(to != f)
            def _():
                remote(src, got.at[f], s.at[i], r.at[f], fs=to, tp=z * 2 + f % 2).wait_send()

    def direct_block(i):
        return 2 * ((f // 2 + i) % (NF // 2)) + c

    def take_direct(b, got, s, r, ms, mr):
        @pl.when(b != f)
        def _():
            remote(got.at[b], got.at[b], s.at[0], r.at[b], fs=b).wait_recv()

        remote(got.at[b], got.at[b], ms.at[b], mr.at[b], tp=z * 2 + 1 - c).start()

    def take_mate(b, got, ms, mr):
        remote(got.at[b], got.at[b], ms.at[b], mr.at[b], tp=z * 2 + 1 - c).wait_recv()

    def wait_mate_sends(got, ms, mr):
        def body(i, carry):
            b = direct_block(i)
            remote(got.at[b], got.at[b], ms.at[b], mr.at[b], tp=z * 2 + 1 - c).wait_send()
            return carry

        lax.fori_loop(0, NF // 2, body, 0)

    along_z(tok_ref, xz, xzs, xzr)

    def send_ids(i, carry):
        remote(idt.at[f], idt.at[f], ids_s.at[i], ids_r.at[f], fs=(f + i) % NF).start()
        return carry

    lax.fori_loop(1, NF, send_ids, 0)

    for load in loads[:4]:
        load.wait()
    halves = [slice(q * LANES, (q + 1) * LANES) for q in range(DS // LANES)]

    def convert_gate_up(i, carry):
        rows = pl.ds(pl.multiple_of(i * ROWS, ROWS), ROWS)
        for q, at in enumerate(halves):
            wg[rows, at] = (wf[q, rows, :] * gain[:, at]).astype(BF16)
            wu[rows, at] = (wf[2 + q, rows, :] * gain[:, at]).astype(BF16)
        return carry

    lax.fori_loop(0, NF, convert_gate_up, 0)

    def reorder_gate_up(h, carry):
        rows = pl.ds(pl.multiple_of(h * E, E), E)
        for q, at in enumerate(halves):
            wgp[rows, at] = (wf[q, pl.ds(h, E, stride=HS), :] * gain[:, at]).astype(BF16)
            wup[rows, at] = (wf[2 + q, pl.ds(h, E, stride=HS), :] * gain[:, at]).astype(BF16)
        return carry


    shared_down = sdt_ref[...].astype(BF16)
    wd[E] = shared_down
    for load in loads[4:]:
        load.wait()

    def convert_down(i, carry):
        rows = pl.ds(pl.multiple_of(i * ROWS, ROWS), ROWS)
        for q, at in enumerate(halves):
            wd[pl.ds(i * EP, EP), :, at] = wf[4 + q, rows, :].reshape(EP, HS, LANES).astype(BF16)
        return carry

    lax.fori_loop(0, NF, convert_down, 0)
    for i in range(LANES // HS):
        wdp[EH + i * HS : EH + (i + 1) * HS, :] = shared_down

    def reorder_down(h, carry):
        rows = pl.ds(pl.multiple_of(h * E, E), E)
        for q, at in enumerate(halves):
            wdp[rows, at] = wf[4 + q, pl.ds(h, E, stride=HS), :].astype(BF16)
        return carry


    def pieces(j, src_of):
        cols = pl.ds(pl.multiple_of(src_of * DS, DS), DS)
        rows = pl.ds(pl.multiple_of(j * ROWS, ROWS), ROWS)
        hid = pl.ds(pl.multiple_of(src_of * HS, HS), HS)
        return (
            (wg.at[rows, :], gs_ref.at[:, cols]),
            (wu.at[rows, :], us_ref.at[:, cols]),
            (wd.at[pl.ds(j * EP, EP)], ds_ref.at[:, hid, :]),
            (ws.at[0:HS, 0:DS], sgs_ref.at[:, cols]),
            (ws.at[HS : 2 * HS, 0:DS], sus_ref.at[:, cols]),
            (wd.at[EP * NF], sds_ref.at[hid, :]),
        )

    def send_weights(which, first, last):
        def body(i, carry):
            j = (f + i + c * (NF - 2 * i)) % NF
            for n, (src, dst) in enumerate(pieces(j, f)):
                if n in which:
                    remote(src, dst, w_s.at[n, i], w_r.at[n, f], fs=j).start()
            return carry

        lax.fori_loop(first, last, body, 0)

    def pair_of(p):
        def block(i):
            late = i // (NF // 2)
            return 2 * ((f // 2 + i) % (NF // 2)) + (c + late) % 2

        return block(2 * p), block(2 * p + 1)

    def take_ids(b):
        @pl.when(b != f)
        def _():
            remote(idt.at[b], idt.at[b], ids_s.at[0], ids_r.at[b], fs=b).wait_recv()

    def compare(p):
        lane = lax.broadcasted_iota(jnp.int32, (TOK, LANES), 1)
        for b in pair_of(p):
            take_ids(b)
            ids = lax.dot_general(
                idt[b], spread_ids[...], TN_DIMS, preferred_element_type=F32
            ).astype(jnp.int32)
            choice[b] = (lane // K) % (LANES // E) * E + ids[:, K * LANES :]
            at = jnp.full((TOK, LANES), -1, jnp.int32)
            for k in range(K):
                at = jnp.where(ids[:, k * LANES : (k + 1) * LANES] == lane % E, lane // E * K + k, at)
            expert[b] = at

    def compare_pairs(n):
        def body(p, carry):
            compare(p)
            return carry

        lax.fori_loop(n * NF // (2 * NZ), (n + 1) * NF // (2 * NZ), body, 0)
        lax.fori_loop(n * HS // NZ, (n + 1) * HS // NZ, reorder_gate_up, 0)
        lax.fori_loop(n * HS // NZ, (n + 1) * HS // NZ, reorder_down, 0)

    send_weights((0,), 1, NF)
    in_plane(tok_ref, xz, xa, xzs, xzr, xps, xpr, compare_pairs)
    send_weights((3, 4, 5), 1, NF)

    square = jnp.square(tok_ref[...].astype(F32))
    for i in range(1, NZ):
        square = square + jnp.square(xz[(z + i) % NZ].astype(F32))
    sq[0] = jnp.broadcast_to(jnp.sum(square, axis=1, keepdims=True), (TOK, LANES))
    swap = remote(sq.at[0], sq.at[1], sq_s, sq_r, tp=z * 2 + 1 - c)
    swap.start()


    for n, (src, dst) in enumerate(pieces(f, f)):
        pltpu.make_async_copy(src, dst, own_sem.at[n]).start()

    def partial(p):
        b0, b1 = pair_of(p)
        x0, x1 = xa[b0], xa[b1]
        x = jnp.concatenate([x0, x1], axis=0)
        step = 4 * LANES
        for n in range(EH // step):
            part = slice(n * step, (n + 1) * step)
            for i, w in enumerate((wgp, wup)):
                y = lax.dot_general(x, w[part, :], NT_DIMS, preferred_element_type=F32)
                for q in range(4):
                    pre[i * TILES + 4 * n + q] = y[:, q * LANES : (q + 1) * LANES]
        per = LANES // (K * (LANES // E))

        lane = lax.broadcasted_iota(jnp.int32, (16, LANES), 1)
        group = lane // (LANES // per)

        def select(m, carry):
            for u in range(4):
                r = 4 * m + u
                rows = pl.ds(pl.multiple_of(r * 16, 16), 16)
                b = b0 + r // (TOK // 16) * (b1 - b0)
                here = pl.ds(pl.multiple_of(r % (TOK // 16) * 16, 16), 16)
                at = choice[b, here]
                for o in range(2 * TILES // per):
                    total = jnp.take_along_axis(pre[o * per, rows], at, axis=1)
                    for j in range(1, per):
                        value = jnp.take_along_axis(pre[o * per + j, rows], at, axis=1)
                        total = jnp.where(group == j, value, total)
                    psend[b, here, o * LANES : (o + 1) * LANES] = total.astype(BF16)
            return carry

        lax.fori_loop(0, 2 * TOK // 64, select, 0)
        half = TOK // 2
        two = jnp.concatenate(
            [
                jnp.concatenate([x0[:half], x1[:half]], axis=0),
                jnp.concatenate([x0[half:], x1[half:]], axis=0),
            ],
            axis=1,
        )
        y = lax.dot_general(two, ws[...], NT_DIMS, preferred_element_type=F32).astype(BF16)
        for q in range(4):
            at = slice(q * LANES, (q + 1) * LANES)
            psend[b0, TOK:, at] = y[16 * q : 16 * q + 16]
            psend[b1, TOK:, at] = y[half + 16 * q : half + 16 * q + 16]

    NX = math.isqrt(NF)
    y, x = f // NX, f % NX
    HALF = (TOK + 16) // 2
    upper, lower = pl.ds(0, HALF), pl.ds(HALF, HALF)

    def upper_copy(b):
        to = y * NX + b % NX
        return remote(
            psend.at[b, upper], qa.at[x, b // NX], p_s.at[0, b], p_r.at[0, x * NX + b // NX], fs=to
        )

    def lower_copy(b):
        to = b // NX * NX + x
        return remote(
            psend.at[b, lower], qb.at[y, b % NX], p_s.at[1, b], p_r.at[1, y * NX + b % NX], fs=to
        )

    def send_partial(b):
        @pl.when(b % NX != x)
        def _():
            upper_copy(b).start()

        @pl.when(b // NX != y)
        def _():
            lower_copy(b).start()

    def add_up(dst, terms):
        for r in range(3):
            at = slice(HALF // 3 * r, HALF // 3 * (r + 1))
            total = terms[0][at].astype(F32)
            for term in terms[1:]:
                total = total + term[at].astype(F32)
            dst[at] = total.astype(dst.dtype)

    def partial_step(p, carry):
        b0, b1 = pair_of(p)
        @pl.when(p < NF // 4)
        def _():
            take_direct(b0, xa, xps, xpr, xms, xmr)
            take_direct(b1, xa, xps, xpr, xms, xmr)

        @pl.when(p >= NF // 4)
        def _():
            take_mate(b0, xa, xms, xmr)
            take_mate(b1, xa, xms, xmr)

        partial(p)
        send_partial(b0)
        send_partial(b1)
        return carry

    lax.fori_loop(0, NF // 2, partial_step, 0)
    swap.wait_recv()

    def second_upper(yb):
        return remote(sa.at[yb], pa.at[y], p2_s.at[0, yb], p2_r.at[0, y], fs=yb * NX + x)

    def second_lower(xb):
        return remote(sb.at[xb], pb.at[x], p2_s.at[1, xb], p2_r.at[1, x], fs=y * NX + xb)

    for i in list(range(1, NX)) + [0]:
        yb, xb = (y + i) % NX, (x + i) % NX
        for j in range(1, NX):
            xs, ys = (x + j) % NX, (y + j) % NX
            remote(
                psend.at[0, upper], qa.at[xs, yb], p_s.at[0, 0], p_r.at[0, xs * NX + yb], fs=f
            ).wait_recv()
            remote(
                psend.at[0, lower], qb.at[ys, xb], p_s.at[1, 0], p_r.at[1, ys * NX + xb], fs=f
            ).wait_recv()
        add_up(
            sa.at[yb],
            [psend.at[yb * NX + x, upper]] + [qa.at[(x + j) % NX, yb] for j in range(1, NX)],
        )
        add_up(
            sb.at[xb],
            [psend.at[y * NX + xb, lower]] + [qb.at[(y + j) % NX, xb] for j in range(1, NX)],
        )
        if i:
            second_upper(yb).start()
            second_lower(xb).start()
    pass
    for i in range(1, NX):
        ys, xs = (y + i) % NX, (x + i) % NX
        remote(sa.at[0], pa.at[ys], p2_s.at[0, 0], p2_r.at[0, ys], fs=f).wait_recv()
        remote(sb.at[0], pb.at[xs], p2_s.at[1, 0], p2_r.at[1, xs], fs=f).wait_recv()
    add_up(ptot.at[upper], [sa.at[y]] + [pa.at[(y + i) % NX] for i in range(1, NX)])
    add_up(ptot.at[lower], [sb.at[x]] + [pb.at[(x + i) % NX] for i in range(1, NX)])

    def summed(mine, got, rows):
        total = mine[f, rows, :].astype(F32)
        for i in range(1, NF):
            total = total + got[(f + i) % NF, rows, :].astype(F32)
        return total

    half = K * HS
    inverse_rms = lax.rsqrt((sq[0] + sq[1]) * (1.0 / D) + NORM_EPS)
    for r in range(TOK // 16):
        rows = slice(16 * r, 16 * r + 16)
        total = ptot[rows, :]
        inv = jnp.concatenate([inverse_rms[rows]] * (half // LANES), axis=1)
        hidden = silu(total[:, :half] * inv) * (total[:, half:] * inv) * wexp[rows, :]
        hv[rows, :] = hidden.astype(BF16)
    lane = lax.broadcasted_iota(jnp.int32, (16, LANES), 1)
    total = ptot[TOK:, :]
    low, high = jnp.zeros((16, LANES), F32), jnp.zeros((16, LANES), F32)
    for q in range(4):
        inv = jnp.where(
            lane < 2 * HS,
            inverse_rms[16 * q : 16 * q + 16],
            inverse_rms[16 * q + TOK // 2 : 16 * q + TOK // 2 + 16],
        )
        pre = total[:, q * LANES : (q + 1) * LANES] * inv
        shared = silu(pre) * pltpu.roll(pre, LANES - HS, 1)
        here = lane // HS == q
        first = pltpu.roll(shared, HS * q, 1) if q else shared
        second = pltpu.roll(shared, (HS * q + 2 * HS) % LANES, 1) if q != 2 else shared
        low = jnp.where(here, first, low)
        high = jnp.where(here, second, high)
    hv[TOK:, :LANES] = low.astype(BF16)
    hv[TOK:, LANES:] = high.astype(BF16)

    along_z(hv, hz, hzs, hzr)
    send_weights((1,), 1, NF)
    send_weights((2,), 1, NF)
    in_plane(hv, hz, ha, hzs, hzr, hps, hpr)

    pass

    def down(p):
        b0, b1 = pair_of(p)
        per = LANES // (K * (LANES // E))

        lane = lax.broadcasted_iota(jnp.int32, (16, LANES), 1)

        def scatter(m, carry):
            for u in range(4):
                r = 4 * m + u
                rows = pl.ds(pl.multiple_of(r * 16, 16), 16)
                b = b0 + r // (TOK // 16) * (b1 - b0)
                s = r % (TOK // 16)
                here = pl.ds(pl.multiple_of(s * 16, 16), 16)
                at = expert[b, here]
                chosen = at >= 0
                at = jnp.maximum(at, 0)
                for o in range(TILES // per):
                    hidden = ha[b, here, o * LANES : (o + 1) * LANES].astype(F32)
                    for j in range(per):
                        value = jnp.take_along_axis(hidden, at + j * (LANES // per), axis=1)
                        asc[o * per + j, rows] = jnp.where(chosen, value, 0.0).astype(BF16)
                tail = ha[b, TOK:, pl.ds(pl.multiple_of(s // 4 * LANES, LANES), LANES)]
                tail_asc[rows] = jnp.where(lane // HS == s % 4, tail.astype(F32), 0.0).astype(BF16)
            return carry

        lax.fori_loop(0, 2 * TOK // 64, scatter, 0)
        y = jnp.dot(
            jnp.concatenate([asc[g] for g in range(TILES)] + [tail_asc[...]], axis=1),
            wdp[...],
            preferred_element_type=F32,
        ).astype(BF16)
        osend[b0] = y[:TOK]
        osend[b1] = y[TOK:]

    def send_out(b):
        @pl.when(b != f)
        def _():
            remote(osend.at[b], orecv.at[f], o_s.at[b], o_r.at[f], fs=b).start()

    def down_step(p, carry):
        b0, b1 = pair_of(p)

        @pl.when(p < NF // 4)
        def _():
            take_direct(b0, ha, hps, hpr, hms, hmr)
            take_direct(b1, ha, hps, hpr, hms, hmr)

        @pl.when(p >= NF // 4)
        def _():
            take_mate(b0, ha, hms, hmr)
            take_mate(b1, ha, hms, hmr)

        down(p)
        send_out(b0)
        send_out(b1)
        return carry

    lax.fori_loop(0, NF // 2, down_step, 0)

    def take_out(i, carry):
        j = (f + i) % NF
        remote(osend.at[j], orecv.at[j], o_s.at[j], o_r.at[j], fs=j).wait_recv()
        return carry

    lax.fori_loop(1, NF, take_out, 0)

    def finish(r, carry):
        rows = pl.ds(pl.multiple_of(r * 16, 16), 16)
        mixed_ref[rows, :] = summed(osend, orecv, rows).astype(BF16)
        return carry

    lax.fori_loop(0, TOK // 16, finish, 0)

    swap.wait_send()
    for n, (src, dst) in enumerate(pieces(f, f)):
        pltpu.make_async_copy(src, dst, own_sem.at[n]).wait()
    wait_spread_sends(tok_ref, xz, xa, xzs, xzr, xps, xpr)
    wait_spread_sends(hv, hz, ha, hzs, hzr, hps, hpr)
    wait_mate_sends(xa, xms, xmr)
    wait_mate_sends(ha, hms, hmr)

    def drain(i, carry):
        j = (f + i) % NF
        remote(idt.at[f], idt.at[f], ids_s.at[i], ids_r.at[f], fs=j).wait_send()
        remote(osend.at[j], orecv.at[f], o_s.at[j], o_r.at[f], fs=j).wait_send()
        for n, (src, dst) in enumerate(pieces(j, f)):
            remote(src, dst, w_s.at[n, i], w_r.at[n, f], fs=j).wait_send()
        for n, (src, dst) in enumerate(pieces(f, j)):
            remote(src, dst, w_s.at[n, i], w_r.at[n, j], fs=j).wait_recv()
        return carry

    lax.fori_loop(1, NF, drain, 0)

    def drain_partial(b, carry):
        @pl.when(b % NX != x)
        def _():
            upper_copy(b).wait_send()

        @pl.when(b // NX != y)
        def _():
            lower_copy(b).wait_send()

        return carry

    lax.fori_loop(0, NF, drain_partial, 0)
    for i in range(1, NX):
        second_upper((y + i) % NX).wait_send()
        second_lower((x + i) % NX).wait_send()


def place(n, *refs):
    src, dst, held, s_in, s_out = refs[:n], refs[n : 2 * n], refs[2 * n : 3 * n], refs[-2], refs[-1]
    parts = []
    for a, b, h in zip(src, dst, held):
        rows = a.shape[0]
        cuts = 4 if rows % 64 == 0 and a.shape[-1] * rows > 1 << 18 else 1
        for i in range(cuts):
            at = pl.ds(rows // cuts * i, rows // cuts)
            parts.append((a.at[at], b.at[at], h.at[at]))
    for i, (a, b, h) in enumerate(parts):
        pltpu.make_async_copy(a, h, s_in.at[i]).start()
    for i, (a, b, h) in enumerate(parts):
        pltpu.make_async_copy(a, h, s_in.at[i]).wait()
        pltpu.make_async_copy(h, b, s_out.at[i]).start()
    for i, (a, b, h) in enumerate(parts):
        pltpu.make_async_copy(h, b, s_out.at[i]).wait()


def solution(mesh):
    NF, NT = mesh.shape["fs"], mesh.shape["tp"]

    def body(tokens, ids, affinity, gain, gt, ut, dt, sgt, sut, sdt):
        TOK, DS = tokens.shape
        E, HS, _ = gt.shape
        EP = E // NF
        EH = E * HS
        NZ = NT // 2
        NX = math.isqrt(NF)
        D = DS * NF
        H = HS * NT
        hbm = pl.BlockSpec(memory_space=pl.ANY)
        vmem = pl.BlockSpec(memory_space=pltpu.VMEM)
        dma = pltpu.SemaphoreType.DMA
        outs = pl.pallas_call(
            functools.partial(kernel, NF, NT, D),
            out_shape=(
                jax.ShapeDtypeStruct((TOK, DS), BF16),
                jax.ShapeDtypeStruct((EP * HS, D), BF16),
                jax.ShapeDtypeStruct((EP * HS, D), BF16),
                jax.ShapeDtypeStruct((EP, H, DS), BF16),
                jax.ShapeDtypeStruct((HS, D), BF16),
                jax.ShapeDtypeStruct((HS, D), BF16),
                jax.ShapeDtypeStruct((H, DS), BF16),
            ),
            in_specs=[vmem] * 4 + [hbm] * 3 + [vmem] * 3,
            out_specs=[vmem] + [hbm] * 6,
            scratch_shapes=[
                pltpu.VMEM((6, EH, LANES), F32),
                pltpu.VMEM((EH, DS), BF16),
                pltpu.VMEM((EH, DS), BF16),
                pltpu.VMEM((E + 1, HS, DS), BF16),
                pltpu.VMEM((LANES, 2 * DS), BF16),
                pltpu.VMEM((EH, DS), BF16),
                pltpu.VMEM((EH, DS), BF16),
                pltpu.VMEM((EH + LANES, DS), BF16),
                pltpu.VMEM((16, (K + 1) * LANES), BF16),
                pltpu.VMEM((TOK, K * HS), F32),
                pltpu.VMEM((NF, 16, TOK), BF16),
                pltpu.VMEM((NZ, TOK, DS), BF16),
                pltpu.VMEM((NF, TOK, DS), BF16),
                pltpu.VMEM((2, TOK, LANES), F32),
                pltpu.VMEM((TOK + 16, K * HS), BF16),
                pltpu.VMEM((NZ, TOK + 16, K * HS), BF16),
                pltpu.VMEM((NF, TOK + 16, K * HS), BF16),
                pltpu.VMEM((NF, TOK, LANES), jnp.int32),
                pltpu.VMEM((NF, TOK, LANES), jnp.int32),
                pltpu.VMEM((2 * EH // LANES, 2 * TOK, LANES), F32),
                pltpu.VMEM((EH // LANES, 2 * TOK, LANES), BF16),
                pltpu.VMEM((2 * TOK, LANES), BF16),
                pltpu.VMEM((NF, TOK + 16, 2 * K * HS), BF16),
                *[pltpu.VMEM((NX, NX, (TOK + 16) // 2, 2 * K * HS), BF16)] * 2,
                *[pltpu.VMEM((NX, (TOK + 16) // 2, 2 * K * HS), BF16)] * 4,
                pltpu.VMEM((TOK + 16, 2 * K * HS), F32),
                pltpu.VMEM((NF, TOK, DS), BF16),
                pltpu.VMEM((NF, TOK, DS), BF16),
                dma((6,)),
                dma((6,)),
                dma((NF,)),
                dma((NF,)),
                *[dma((NZ,)), dma((NZ,)), dma((NZ,)), dma((NF,)), dma((NF,)), dma((NF,))] * 2,
                *[dma((2, NF))] * 2,
                *[dma((2, NX))] * 2,
                *[dma((NF,))] * 2,
                dma((6, NF)),
                dma((6, NF)),
                dma,
                dma,
            ],
            compiler_params=pltpu.CompilerParams(
                collective_id=0,
                has_side_effects=True,
                vmem_limit_bytes=60 * 1024 * 1024,
            ),
        )(
            tokens, ids.T, affinity.T, gain.reshape(1, DS),
            gt.reshape(EH, DS), ut.reshape(EH, DS), dt.reshape(EH, DS), sgt, sut, sdt,
        )
        n = len(outs)
        outs = (*outs[:3], outs[3].reshape(EP * H, DS), *outs[4:])
        shapes = [jax.ShapeDtypeStruct(a.shape, a.dtype) for a in outs]
        outs = pl.pallas_call(
            functools.partial(place, n),
            out_shape=shapes,
            in_specs=[hbm] * n,
            out_specs=[hbm] * n,
            scratch_shapes=[pltpu.VMEM(a.shape, a.dtype) for a in shapes] + [dma((4 * n,))] * 2,
            compiler_params=pltpu.CompilerParams(vmem_limit_bytes=60 * 1024 * 1024),
        )(*outs)
        mixed, gs, us, ds, sgs, sus, sds = outs
        ds = ds.reshape(EP, H, DS)
        return mixed, gs.reshape(EP, HS, D), us.reshape(EP, HS, D), ds, sgs, sus, sds

    return jax.shard_map(
        body,
        mesh=mesh,
        in_specs=(
            P("fs", "tp"),
            P("fs", None),
            P("fs", None),
            P("fs"),
            P(None, "tp", "fs"),
            P(None, "tp", "fs"),
            P(None, "fs", "tp"),
            P("tp", "fs"),
            P("tp", "fs"),
            P("fs", "tp"),
        ),
        out_specs=(
            P("fs", "tp"),
            P("fs", "tp", None),
            P("fs", "tp", None),
            P("fs", None, "tp"),
            P("tp", None),
            P("tp", None),
            P(None, "tp"),
        ),
        check_vma=False,
    )
```
